32 devices in a mesh: sp: 16 (over z, y, x), tp: 2 (over core).
Axes of the slice: x: 2, y: 2, z: 4, core: 2. Of those that a mesh axis runs over, the one named last changes fastest.
Arguments:
- stream: bfloat16 [4096, 2048], P('sp', 'tp'), may hold values from -6 to 6
- out_grad: bfloat16 [4096, 2048], P('sp', 'tp'), may hold values from -6 to 6
- gate_in: bfloat16 [4096, 1024], P('sp', 'tp'), may hold values from -6 to 6
- conv_gate: bfloat16 [4096, 1024], P('sp', 'tp'), may hold values from -6 to 6
- conv_value: bfloat16 [4096, 1024], P('sp', 'tp'), may hold values from -6 to 6
- taps: float32 [3, 1024], P(None, 'tp'), may hold values from -3.5 to 3.5
- w_out: bfloat16 [2048, 1024], P(None, 'tp'), may hold values from -0.1875 to 0.1875
- route_ids: int32 [4096, 2], P('sp'), may hold values from 0 to 15, all different within a row; in each aligned block of 256 rows (0 to 255, 256 to 511, ...) at most 64 rows name the same one
- route_weights: float32 [4096, 2], P('sp'), may hold values from 0.1 to 1
- w_gate: bfloat16 [16, 2048, 1024], P('sp', None, 'tp'), may hold values from -0.125 to 0.125
- w_up: bfloat16 [16, 2048, 1024], P('sp', None, 'tp'), may hold values from -0.125 to 0.125
- w_down: bfloat16 [16, 1024, 2048], P('sp', 'tp'), may hold values from -0.1875 to 0.1875
Outputs:
- stream_grad: bfloat16 [4096, 2048], P('sp', 'tp')
- gate_in_grad: bfloat16 [4096, 1024], P('sp', 'tp')
- conv_gate_grad: bfloat16 [4096, 1024], P('sp', 'tp')
- conv_value_grad: bfloat16 [4096, 1024], P('sp', 'tp')
- w_out_grad: float32 [2048, 1024], P('sp', 'tp')
- w_gate_grad: float32 [16, 2048, 1024], P('sp', None, 'tp')
- w_up_grad: float32 [16, 2048, 1024], P('sp', None, 'tp')
- w_down_grad: float32 [16, 1024, 2048], P('sp', 'tp')
The draws below stay inside these ranges and needn't reach their ends.
Inputs may be any that keep to these rules, and one draw needn't show every extreme that they name: `route_ids`: the ids of one token differ. Within each aligned block of 256 tokens (the rows of one index of sp), no expert is named by more than 64 routes, and in every draw some expert is named by exactly 64 routes of some block.
All inputs are finite; a program needn't handle non-finite values.
Results may differ from the reference program's by a relative error of at most 0.009.
Values may be sent and summed in bfloat16 or wider, within the bound.
A program may use at most 128 MiB of HBM per device.

```python
import math
import jax
import jax.numpy as jnp
import numpy as np
from jax import lax

D = 2048
CW = 1024
FF = 1024
TOP = 2
TAPS = 3
EXPERTS = 16
TOK_DEV = 256
TOKENS = 4096
CAP = 64
EXPERT_ROWS = 1024
N_SP = 16
N_TP = 2


def strengthened(drawn, rng, source, target, parts, factor):
    owner, partner = [(jnp.arange(drawn.shape[position]) // (drawn.shape[position] // parts)).reshape([-1 if axis == position else 1 for axis in range(drawn.ndim)]) for position in (source, target)]
    chosen = jax.random.permutation(rng, parts)[partner]
    strong = (owner == chosen) | (owner == (partner + parts // 2) % parts)
    return jnp.where(strong, factor * drawn, drawn)


def level_of(own_key, dims, pieces, smallest, high):
    def one(position, blocks):
        steps = jax.random.uniform(jax.random.fold_in(jax.random.fold_in(own_key, 6), position), (blocks,), jnp.float32, smallest / len(pieces), high / len(pieces))
        return jnp.repeat(jnp.exp(steps), dims[position] // blocks).reshape((-1,) + (1,) * (len(dims) - position - 1))

    factor_of = one(*pieces[0])
    for cut in pieces[1:]:
        factor_of = factor_of * one(*cut)
    return factor_of


def deal_out(stream_key, own, number, rows, count, top, bound, lean):
    ranking = jax.random.permutation(stream_key, count)
    packed, usual = shares(count, rows * top, bound, lean, True), shares(count, rows * top, bound, lean, False)
    places = jnp.arange(count)

    def named(sizes, turn):
        used = int((sizes > 0).sum())
        fixed = max(1, used // 4)
        passed = fixed + (places - fixed + turn * (used - fixed)) % max(1, count - fixed)
        return jnp.zeros((count,), jnp.int32).at[ranking[jnp.where(places < fixed, places, passed)]].set(jnp.asarray(sizes, jnp.int32))

    sizes = jnp.where(number % 4 == 0, named(packed, number // 4), named(usual, number - number // 4 - 1))
    mixed = jax.random.permutation(jax.random.fold_in(own, 3), count)
    giver, taker = mixed[0:count // 2 * 2:2], mixed[1:count // 2 * 2:2]
    room = jnp.minimum(sizes[giver] - 1, bound - sizes[taker]) // 2
    room = jnp.where((giver == ranking[0]) | (taker == ranking[0]) | (sizes[taker] == 0), 0, jnp.maximum(room, 0))
    passed = jax.random.randint(jax.random.fold_in(own, 4), (count // 2,), 0, 1 << 20) % (room + 1)
    sizes = sizes.at[giver].add(-passed).at[taker].add(passed)
    items = jnp.searchsorted(jnp.cumsum(sizes), jnp.arange(rows * top), side="right").astype(jnp.int32)
    listing = items.reshape(top, rows).T
    listing = listing[jax.random.permutation(jax.random.fold_in(own, 1), rows)]
    turn = jax.random.randint(jax.random.fold_in(own, 2), (rows, 1), 0, top)
    return jnp.take_along_axis(listing, (jnp.arange(top)[None, :] + turn) % top, axis=1)


def shares(amount, total, most, skew, full):
    loads = [(1 << 20) // math.isqrt(grade ** skew) + 1 for grade in range(1, amount + 1)]
    largest = most if full else min(most, max(-(-total // amount), total * loads[0] // sum(loads)))
    least = 1 if total - largest >= amount - 1 else 0
    given, rest = [largest] + [least] * (amount - 1), total - largest - least * (amount - 1)
    while rest > 0:
        free = [i for i in range(1, amount) if given[i] < largest] or [i for i in range(1, amount) if given[i] < most]
        whole, left = sum([loads[i] for i in free]), rest
        for i in free:
            addition = min(most - given[i], max(1, left * loads[i] // whole), rest)
            given[i] = given[i] + addition
            rest = rest - addition
    return np.array(given)


def scatter_about(own_key, dims, scale, limit, split=(), kind=jnp.bfloat16):
    array = scale * jax.random.normal(own_key, dims, jnp.float32)
    if split:
        array = array * level_of(own_key, dims, split, -0.22, 0.18)
    return jnp.clip(array, -limit, limit).astype(kind)


def gaussian_with(rng, extent, width, most, pieces, heavy, held_as=jnp.bfloat16):
    result = width * jax.random.normal(rng, extent, jnp.float32)
    if pieces:
        result = result * level_of(rng, extent, pieces, -0.22, 0.18)
    return jnp.clip(strengthened(result, jax.random.fold_in(rng, 3), *heavy), -most, most).astype(held_as)


def setup_inputs(seed: int = 0) -> dict:
    key_list = jax.random.split(jax.random.key(seed), 13)
    stream = scatter_about(key_list[0], (TOKENS, D), 1.0, 6.0, ((0, 16), (1, 2)))
    out_grad = gaussian_with(key_list[1], (TOKENS, D), 1.0, 6.0, ((0, 16), (1, 2)), (0, 1, 16, 2.0))
    gate_in = scatter_about(key_list[2], (TOKENS, CW), 1.0, 6.0, ((0, 16), (1, 2)))
    conv_gate = scatter_about(key_list[3], (TOKENS, CW), 1.0, 6.0, ((0, 16), (1, 2)))
    conv_value = scatter_about(key_list[4], (TOKENS, CW), 1.0, 6.0, ((0, 16), (1, 2)))
    taps = scatter_about(key_list[5], (TAPS, CW), TAPS ** -0.5, 3.5, ((1, 2),), jnp.float32)
    w_out = scatter_about(key_list[6], (D, CW), CW ** -0.5, 0.1875, ((1, 2),))
    route_ids_keys = jax.random.split(jax.random.fold_in(key_list[7], 1), TOKENS // TOK_DEV)
    route_ids_turns = jax.random.permutation(jax.random.fold_in(key_list[7], 3), TOKENS // TOK_DEV)
    route_ids = jax.vmap(lambda own, number: deal_out(jax.random.fold_in(key_list[7], 2), own, number, TOK_DEV, EXPERTS, TOP, CAP, 2))(route_ids_keys, route_ids_turns).reshape((TOKENS, TOP))
    route_weights = jnp.clip(0.1 + 0.9 * jax.random.uniform(key_list[8], (TOKENS, TOP), jnp.float32) ** level_of(key_list[8], (TOKENS, TOP), ((0, 16),), -0.2, 0.2), 0.1, 1.0)
    w_gate = scatter_about(key_list[9], (EXPERTS, D, FF), D ** -0.5, 0.125, ((0, 16), (2, 2)))
    w_up = scatter_about(key_list[10], (EXPERTS, D, FF), D ** -0.5, 0.125, ((0, 16), (2, 2)))
    w_down = scatter_about(key_list[11], (EXPERTS, FF, D), FF ** -0.5, 0.1875, ((0, 16), (1, 2)))
    return {"stream": stream, "out_grad": out_grad, "gate_in": gate_in, "conv_gate": conv_gate, "conv_value": conv_value, "taps": taps, "w_out": w_out, "route_ids": route_ids, "route_weights": route_weights, "w_gate": w_gate, "w_up": w_up, "w_down": w_down}


def expert_step(carry_rows, stream_pad, cot_pad):
    table_row, gate_weight, up_weight, down_weight = carry_rows
    routes_total = TOKENS * TOP
    token_index = jnp.where(table_row < routes_total, table_row // TOP, TOKENS).astype(jnp.int32)
    expert_in = stream_pad[token_index]
    expert_cot = cot_pad[table_row]
    pre_gate = jnp.dot(expert_in, gate_weight, preferred_element_type=jnp.float32)
    pre_up = jnp.dot(expert_in, up_weight, preferred_element_type=jnp.float32)
    sigmoid_gate = jax.nn.sigmoid(pre_gate)
    silu_gate = pre_gate * sigmoid_gate
    hidden = (silu_gate * pre_up).astype(jnp.bfloat16)
    hidden_grad = jnp.dot(expert_cot, down_weight.T, preferred_element_type=jnp.float32)
    down_grad = jnp.dot(hidden.T, expert_cot, preferred_element_type=jnp.float32)
    up_grad = (hidden_grad * silu_gate).astype(jnp.bfloat16)
    gate_grad = (hidden_grad * pre_up * sigmoid_gate * (1.0 + pre_gate * (1.0 - sigmoid_gate))).astype(jnp.bfloat16)
    gate_w_grad = jnp.dot(expert_in.T, gate_grad, preferred_element_type=jnp.float32)
    up_w_grad = jnp.dot(expert_in.T, up_grad, preferred_element_type=jnp.float32)
    block_width = FF // N_TP
    running = jnp.zeros((EXPERT_ROWS, D), jnp.float32)
    for block_index in range(N_TP):
        lower = block_index * block_width
        upper = lower + block_width
        partial_term = jnp.dot(gate_grad[:, lower:upper], gate_weight[:, lower:upper].T, preferred_element_type=jnp.float32)
        partial_term = partial_term + jnp.dot(up_grad[:, lower:upper], up_weight[:, lower:upper].T, preferred_element_type=jnp.float32)
        rounded = lax.optimization_barrier(partial_term.astype(jnp.bfloat16))
        running = running + rounded.astype(jnp.float32)
    return gate_w_grad, up_w_grad, down_grad, running.astype(jnp.bfloat16)


def reference(stream, out_grad, gate_in, conv_gate, conv_value, taps, w_out, route_ids, route_weights, w_gate, w_up, w_down):
    prod_rows = conv_gate.astype(jnp.float32) * conv_value.astype(jnp.float32)
    padded = jnp.concatenate([jnp.zeros((TAPS - 1, CW), jnp.float32), prod_rows], axis=0)
    conv_sum = jnp.zeros((TOKENS, CW), jnp.float32)
    for tap_index in range(TAPS):
        conv_sum = conv_sum + taps[tap_index][None, :] * padded[tap_index:tap_index + TOKENS]
    mixer_out = (gate_in.astype(jnp.float32) * conv_sum).astype(jnp.bfloat16)

    routes_dev = TOK_DEV * TOP
    route_block = route_ids.reshape(N_SP, routes_dev)
    one_hot = (route_block[:, :, None] == jnp.arange(EXPERTS, dtype=jnp.int32)[None, None, :]).astype(jnp.int32)
    slot_pos = jnp.sum(jnp.cumsum(one_hot, axis=1) * one_hot, axis=2) - 1
    source_index = jnp.arange(N_SP, dtype=jnp.int32)[:, None]
    flat_slot = (route_block * EXPERT_ROWS + source_index * CAP + slot_pos).reshape(-1).astype(jnp.int32)
    routes_total = TOKENS * TOP
    table = jnp.full((EXPERTS * EXPERT_ROWS,), routes_total, jnp.int32)
    table = table.at[flat_slot].set(jnp.arange(routes_total, dtype=jnp.int32))
    table = table.reshape(EXPERTS, EXPERT_ROWS)

    stream_pad = jnp.concatenate([stream, jnp.zeros((1, D), jnp.bfloat16)], axis=0)
    scaled = (route_weights[:, :, None] * out_grad[:, None, :].astype(jnp.float32)).astype(jnp.bfloat16)
    cot_pad = jnp.concatenate([scaled.reshape(routes_total, D), jnp.zeros((1, D), jnp.bfloat16)], axis=0)

    def per_expert(carry_rows):
        return expert_step(carry_rows, stream_pad, cot_pad)

    w_gate_grad, w_up_grad, w_down_grad, row_grad = lax.map(per_expert, (table, w_gate, w_up, w_down))
    row_flat = row_grad.reshape(EXPERTS * EXPERT_ROWS, D)
    route_rows = row_flat[flat_slot].astype(jnp.float32).reshape(TOKENS, TOP, D)
    input_grad = jnp.sum(route_rows, axis=1)
    stream_grad = (out_grad.astype(jnp.float32) + input_grad).astype(jnp.bfloat16)

    w_out_grad = jnp.dot(stream_grad.T, mixer_out, preferred_element_type=jnp.float32)
    mixer_grad = jnp.dot(stream_grad, w_out, preferred_element_type=jnp.float32).astype(jnp.bfloat16)
    gate_in_grad = (mixer_grad.astype(jnp.float32) * conv_sum).astype(jnp.bfloat16)
    conv_inner = mixer_grad.astype(jnp.float32) * gate_in.astype(jnp.float32)
    padded_back = jnp.concatenate([conv_inner, jnp.zeros((TAPS - 1, CW), jnp.float32)], axis=0)
    prod_grad = jnp.zeros((TOKENS, CW), jnp.float32)
    for tap_index in range(TAPS):
        offset = TAPS - 1 - tap_index
        prod_grad = prod_grad + taps[tap_index][None, :] * padded_back[offset:offset + TOKENS]
    conv_gate_grad = (prod_grad * conv_value.astype(jnp.float32)).astype(jnp.bfloat16)
    conv_value_grad = (prod_grad * conv_gate.astype(jnp.float32)).astype(jnp.bfloat16)
    return (stream_grad, gate_in_grad, conv_gate_grad, conv_value_grad, w_out_grad, w_gate_grad, w_up_grad, w_down_grad)
```

```python
import functools

import jax
import jax.numpy as jnp
from jax import lax
from jax.experimental import pallas as pl
from jax.experimental.pallas import tpu as pltpu
from jax.sharding import PartitionSpec as P

MESH = pl.DeviceIdType.MESH
LAYERS = 4
PARTS = 4
CHUNKS = 4
F32 = jnp.float32
BF16 = jnp.bfloat16
OWN, NEXT, ACROSS, FAR = 0, 1, 2, 3


def passed_along(shard, axis, by):
    count = lax.axis_size(axis)
    pairs = [(i, i + by) for i in range(count) if 0 <= i + by < count]
    return lax.ppermute(shard, axis, pairs)


def dot(a, b, ca, cb):
    return lax.dot_general(a, b, (((ca,), (cb,)), ((), ())), preferred_element_type=F32)


def team_size(count):
    size = 1
    while size * size < count:
        size *= 2
    return size


def expert_kernel(
    count,
    cap,
    stream_in,
    grad_in,
    ids,
    weights,
    gate_in,
    conv_gate,
    conv_value,
    taps,
    wg_hbm,
    wu_hbm,
    wd_hbm,
    half_out,
    conv_out,
    mix_out,
    gate_out,
    up_out,
    down_out,
    toks_in,
    table,
    pick,
    scale,
    rel,
    rows,
    cot,
    wg,
    wu,
    wd,
    pre_g,
    pre_u,
    hidden,
    gg,
    ug,
    part_out,
    part_in,
    ret,
    back,
    col_out,
    col_in,
    total,
    gate_f,
    up_f,
    down_f,
    mix,
    mix_src,
    padded,
    halo_src,
    halo_dst,
    w_sem,
    out_sem,
    z_send,
    z_recv,
    t_send,
    t_recv,
    i_send,
    i_recv,
    f_send,
    f_recv,
    p_send,
    p_recv,
    r_send,
    r_recv,
    c_send,
    c_recv,
    m_send,
    m_recv,
    h_sem,
):
    me = lax.axis_index("sp")
    half = lax.axis_index("tp")
    other = 1 - half
    team = count // LAYERS
    place, layer = lax.rem(me, team), me // team
    side = layer // 2
    inner = lax.rem(layer + 1, LAYERS) >= 2
    outer = jnp.logical_not(inner)
    next_layer = layer + 1 - 2 * lax.rem(layer, 2)
    across_layer = 2 - side
    far_layer = 3 * (1 - side)
    toks, width = stream_in.shape
    slots = team * cap
    depth = taps.shape[0]
    top = ids.shape[0]

    def column(at):
        return (at * team + place, half)

    def teammate(i):
        return layer * team + lax.rem(place + i, team)

    loads = []
    for n, (a, b) in enumerate(((wg_hbm, wg), (wu_hbm, wu), (wd_hbm, wd))):
        load = pltpu.make_async_copy(a.at[0], b, w_sem.at[n])
        load.start()
        loads.append(load)

    after, before = lax.rem(me + 1, count), lax.rem(me + count - 1, count)
    barrier = pltpu.get_barrier_semaphore()

    def greet(device):
        pl.semaphore_signal(barrier, inc=1, device_id=device, device_id_type=MESH)

    greet(column(lax.rem(layer + 1, LAYERS)))
    greet(column(lax.rem(layer + 2, LAYERS)))
    greet(column(lax.rem(layer + 3, LAYERS)))

    @pl.loop(1, team)
    def _(i):
        greet((teammate(i), half))

    greet((me, other))
    greet((after, half))
    greet((before, half))
    pl.semaphore_wait(barrier, LAYERS - 1 + team - 1 + 3)

    def remote(src, dst, send, recv, device):
        return pltpu.make_async_remote_copy(
            src_ref=src,
            dst_ref=dst,
            send_sem=send,
            recv_sem=recv,
            device_id=device,
            device_id_type=MESH,
        )

    def block(k):
        return pl.ds(pl.multiple_of(k * cap, cap), cap)

    def piece(j, k):
        return pl.ds(pl.multiple_of(j * slots + k * cap, cap), cap)

    def group(j):
        return pl.ds(j * slots, slots)

    whole = (stream_in, grad_in)

    def blocks_of(which, j):
        return whole[which] if j == OWN else toks_in.at[which, j - 1]

    stretch = toks // CHUNKS

    def hop(which, n, j, to, lands, c):
        at = pl.ds(c * stretch, stretch)
        return remote(
            blocks_of(which, j).at[at],
            toks_in.at[which, lands - 1, at],
            z_send.at[which, n, c],
            z_recv.at[which, lands - 1, c],
            column(to),
        )

    def own_to_next(which, c):
        return hop(which, 0, OWN, next_layer, NEXT, c)

    def own_to_across(which, c):
        return hop(which, 1, OWN, across_layer, ACROSS, c)

    def next_to_across(which, c):
        return hop(which, 2, NEXT, across_layer, FAR, c)

    def across_to_next(which, c):
        return hop(which, 3, ACROSS, next_layer, ACROSS, c)

    def far_to_next(which, c):
        return hop(which, 4, FAR, next_layer, FAR, c)

    def arrived(which, j):
        for c in range(CHUNKS):
            hop(which, 0, j, next_layer, j, c).wait_recv()

    def begin(copy, which):
        for c in range(CHUNKS):
            copy(which, c).start()

    def relay(*steps):
        for c in range(CHUNKS):
            for which, j, copy in steps:
                hop(which, 0, j, next_layer, j, c).wait_recv()
                copy(which, c).start()

    last = pl.ds(toks - 8, 8)
    halo_src[...] = conv_gate[last].astype(F32) * conv_value[last].astype(F32)
    halo = remote(halo_src, halo_dst, h_sem.at[0], h_sem.at[1], (after, half))
    halo.start()
    begin(own_to_next, 0)

    @pl.when(inner)
    def _():
        begin(own_to_across, 0)

    expert = lax.broadcasted_iota(jnp.int32, (count, toks), 0)
    hits = [ids[k : k + 1] == expert for k in range(top)]
    named = functools.reduce(jnp.logical_or, hits)
    named = jnp.where(named, 1.0, 0.0).astype(BF16)
    early = lax.broadcasted_iota(jnp.int32, (toks, toks), 0)
    late = lax.broadcasted_iota(jnp.int32, (toks, toks), 1)
    earlier = jnp.where(early < late, 1.0, 0.0).astype(BF16)
    spots = dot(named, earlier, 1, 0) + (expert * cap).astype(F32)
    table[OWN] = jnp.zeros(table.shape[1:], F32)
    for k in range(top):
        table[OWN, k : k + 1] = jnp.sum(jnp.where(hits[k], spots, 0.0), axis=0, keepdims=True)
        table[OWN, top + k : top + k + 1] = weights[k : k + 1]

    seen_as = jnp.where(inner, ACROSS, FAR)

    def table_copy(n, to, lands):
        return remote(
            table.at[OWN], table.at[lands], t_send.at[n], t_recv.at[lands], column(to)
        )

    tables = (
        table_copy(0, next_layer, NEXT),
        table_copy(1, across_layer, seen_as),
        table_copy(2, far_layer, seen_as),
    )
    for copy in tables:
        copy.start()

    begin(own_to_next, 1)

    base = (layer * slots).astype(F32)

    def choose(j):
        spot = lax.broadcasted_iota(jnp.int32, (slots, toks), 0).astype(F32)
        found = [table[j, k : k + 1] - base == spot for k in range(top)]
        pick[j] = jnp.where(functools.reduce(jnp.logical_or, found), 1.0, 0.0).astype(BF16)
        scale[j] = sum(
            jnp.sum(
                jnp.where(found[k], table[j, top + k : top + k + 1], 0.0), axis=1, keepdims=True
            )
            for k in range(top)
        )

    bufs = (rows, cot)

    def in_copy(which, j, i):
        return remote(
            rel.at[which, j, block(lax.rem(place + i, team))],
            bufs[which].at[half, piece(j, place)],
            i_send.at[which, j, i],
            i_recv.at[which, j, i],
            (teammate(i), half),
        )

    def in_arrival(which, j, i):
        at = bufs[which].at[half, piece(j, lax.rem(place - i + team, team))]
        return remote(at, at, i_send.at[which, j, i], i_recv.at[which, j, i], (teammate(i), half))

    def pass_copy(which, j, i):
        at = bufs[which].at[half, piece(j, lax.rem(place - i + team, team))]
        return remote(at, at, f_send.at[which, j, i], f_recv.at[which, j, i], (me, other))

    def own_pass(which, j):
        return remote(
            rel.at[which, j, block(place)],
            bufs[which].at[half, piece(j, place)],
            f_send.at[which, j, 0],
            f_recv.at[which, j, 0],
            (me, other),
        )

    def deal(which, j):
        chosen = dot(pick[j], blocks_of(which, j)[...], 1, 0)
        if which == 1:
            chosen = scale[j] * chosen
        rel[which, j] = chosen.astype(BF16)

        @pl.loop(1, team)
        def _(i):
            in_copy(which, j, i).start()

        own_pass(which, j).start()
        bufs[which][half, piece(j, place)] = rel[which, j, block(place)]

    def gather(which, j):
        @pl.loop(1, team)
        def _(i):
            in_arrival(which, j, i).wait_recv()
            pass_copy(which, j, i).start()

        @pl.loop(0, team)
        def _(i):
            pass_copy(which, j, i).wait_recv()

    mine_at = pl.ds(pl.multiple_of(half * width, width), width)
    other_at = pl.ds(pl.multiple_of(other * width, width), width)

    def part_copy(j):
        return remote(
            part_out.at[group(j)], part_in.at[group(j)], p_send.at[j], p_recv.at[j], (me, other)
        )

    def ret_copy(j, i):
        return remote(
            ret.at[piece(j, lax.rem(place + i, team))],
            back.at[piece(j, place)],
            r_send.at[j, i],
            r_recv.at[j, i],
            (teammate(i), half),
        )

    def ret_arrival(j, i):
        at = back.at[piece(j, lax.rem(place - i + team, team))]
        return remote(at, at, r_send.at[j, i], r_recv.at[j, i], (teammate(i), half))

    def ahead(j):
        gather(0, j)
        at = group(j)
        left, right = rows[0, at], rows[1, at]
        pre_g[at] = dot(left, wg[:width], 1, 0) + dot(right, wg[width:], 1, 0)
        pre_u[at] = dot(left, wu[:width], 1, 0) + dot(right, wu[width:], 1, 0)

    def behind(j):
        gather(1, j)
        at = group(j)
        grad = dot(cot[0, at], wd[:, :width], 1, 1) + dot(cot[1, at], wd[:, width:], 1, 1)
        pg, pu = pre_g[at], pre_u[at]
        sig = jax.nn.sigmoid(pg)
        silu = pg * sig
        hidden[at] = (silu * pu).astype(BF16)
        ug_now = (grad * silu).astype(BF16)
        gg_now = (grad * pu * sig * (1.0 + pg * (1.0 - sig))).astype(BF16)
        ug[at] = ug_now
        gg[at] = gg_now
        far = dot(gg_now, wg[other_at], 1, 1) + dot(ug_now, wu[other_at], 1, 1)
        part_out[at] = far.astype(BF16)
        part_copy(j).start()
        near = dot(gg_now, wg[mine_at], 1, 1) + dot(ug_now, wu[mine_at], 1, 1)
        near = near.astype(BF16).astype(F32)
        part_copy(j).wait_recv()
        ret[at] = (near + part_in[at].astype(F32)).astype(BF16)

        @pl.loop(1, team)
        def _(i):
            ret_copy(j, i).start()

        back[piece(j, place)] = ret[piece(j, place)]

    def returned(j):
        @pl.loop(1, team)
        def _(i):
            ret_arrival(j, i).wait_recv()

    share = width // PARTS

    def cols(n):
        return pl.ds(n * share, share)

    def sum_copy(j, n):
        if j == NEXT:
            to, lands = next_layer, 0
        else:
            to = jnp.where(inner, across_layer, next_layer)
            lands = jnp.where(inner, j - 1, j + 1)
        return remote(
            col_out.at[j - 1, :, cols(n)],
            col_in.at[lands, :, cols(n)],
            c_send.at[j - 1, n],
            c_recv.at[lands, n],
            column(to),
        )

    def sum_arrival(lands, n):
        at = col_in.at[lands, :, cols(n)]
        return remote(at, at, c_send.at[0, n], c_recv.at[lands, n], column(next_layer))

    def partial(j, n):
        return dot(pick[j], back[group(j), cols(n)], 0, 0)

    def send_sums(j):
        for n in range(PARTS):
            col_out[j - 1, :, cols(n)] = partial(j, n).astype(BF16)
            sum_copy(j, n).start()

    def forward_sums(*js):
        for n in range(PARTS):
            for j in js:
                mine = partial(j, n)
                sum_arrival(j + 1, n).wait_recv()
                mine = mine + col_in[j + 1, :, cols(n)].astype(F32)
                col_out[j - 1, :, cols(n)] = mine.astype(BF16)
                sum_copy(j, n).start()

    choose(OWN)
    deal(0, OWN)
    deal(1, OWN)

    halo.wait_recv()
    prod = conv_gate[...].astype(F32) * conv_value[...].astype(F32)
    padded[8:] = prod
    padded[:8] = jnp.where(me == 0, 0.0, halo_dst[...])
    conv = jnp.zeros(prod.shape, F32)
    for tap in range(depth):
        start = 8 - (depth - 1) + tap
        conv = conv + taps[tap : tap + 1] * padded[start : start + toks]
    conv_out[...] = conv
    mix_src[...] = (gate_in[...].astype(F32) * conv).astype(BF16)

    crew = team_size(count)
    seat = lax.rem(me, crew)

    def mix_copy(j):
        return remote(
            mix_src,
            mix.at[pl.ds(pl.multiple_of(j * toks, toks), toks)],
            m_send.at[j],
            m_recv.at[j],
            (me - seat + lax.rem(seat + j, crew), half),
        )

    def informed(j):
        table_copy(0, next_layer, j).wait_recv()
        choose(j)

    @pl.when(inner)
    def _():
        relay((0, NEXT, next_to_across), (0, ACROSS, across_to_next))

    @pl.when(outer)
    def _():
        arrived(0, NEXT)

    informed(NEXT)
    deal(0, NEXT)
    for load in loads:
        load.wait()

    @pl.when(inner)
    def _():
        relay((1, NEXT, next_to_across), (0, FAR, far_to_next))
        begin(own_to_across, 1)

    @pl.when(outer)
    def _():
        arrived(1, NEXT)

    deal(1, NEXT)
    ahead(OWN)
    behind(OWN)

    @pl.when(inner)
    def _():
        relay((1, FAR, far_to_next))

    ahead(NEXT)
    behind(NEXT)

    @pl.when(outer)
    def _():
        arrived(0, ACROSS)

    informed(ACROSS)
    deal(0, ACROSS)
    returned(OWN)
    total[...] = dot(pick[OWN], back[group(OWN)], 0, 0)
    returned(NEXT)

    @pl.when(outer)
    def _():
        send_sums(NEXT)
        arrived(0, FAR)

    informed(FAR)
    deal(0, FAR)

    @pl.when(inner)
    def _():
        relay((1, ACROSS, across_to_next))

    ahead(ACROSS)

    @pl.when(outer)
    def _():
        arrived(1, FAR)

    deal(1, FAR)
    ahead(FAR)

    @pl.when(outer)
    def _():
        arrived(1, ACROSS)

    deal(1, ACROSS)
    behind(FAR)
    behind(ACROSS)

    @pl.loop(1, crew)
    def _(j):
        mix_copy(j).start()

    mix[pl.ds(0, toks)] = mix_src[...]
    returned(FAR)

    @pl.when(outer)
    def _():
        send_sums(FAR)

    hid_tile = min(256, hidden.shape[1])

    @pl.loop(0, hidden.shape[1] // hid_tile)
    def _(t):
        to = pl.ds(pl.multiple_of(t * hid_tile, hid_tile), hid_tile)
        x = hidden[:, to].T
        for h in range(2):
            down_f[to, h * width : (h + 1) * width] = dot(x, cot[h], 1, 0).astype(BF16)

    stores = [pltpu.make_async_copy(down_f, down_out.at[0], out_sem.at[2])]
    stores[-1].start()

    tile = 256
    per_half = width // tile

    @pl.loop(0, 2 * per_half)
    def _(t):
        h, c = t // per_half, lax.rem(t, per_half)
        at = pl.ds(pl.multiple_of(c * tile, tile), tile)
        to = pl.ds(pl.multiple_of(t * tile, tile), tile)
        x = rows[h, :, at].T
        gate_f[to] = dot(x, gg[...], 1, 0).astype(BF16)
        up_f[to] = dot(x, ug[...], 1, 0).astype(BF16)

    stores.append(pltpu.make_async_copy(gate_f, gate_out.at[0], out_sem.at[0]))
    stores.append(pltpu.make_async_copy(up_f, up_out.at[0], out_sem.at[1]))
    for store in stores[1:]:
        store.start()

    returned(ACROSS)

    @pl.when(outer)
    def _():
        send_sums(ACROSS)

    @pl.when(inner)
    def _():
        forward_sums(FAR)
        forward_sums(NEXT, ACROSS)

        for n in range(PARTS):
            sum_arrival(1, n).wait_recv()
            total[:, cols(n)] += col_in[1, :, cols(n)].astype(F32)

    for n in range(PARTS):
        sum_arrival(0, n).wait_recv()
        now = total[:, cols(n)] + col_in[0, :, cols(n)].astype(F32)
        half_out[:, cols(n)] = (grad_in[:, cols(n)].astype(F32) + now).astype(BF16)

    for which in range(2):
        for c in range(CHUNKS):
            own_to_next(which, c).wait_send()

        for j in range(LAYERS):
            own_pass(which, j).wait_send()

            @pl.loop(1, team)
            def _(i):
                in_copy(which, j, i).wait_send()
                pass_copy(which, j, i).wait_send()

    @pl.when(inner)
    def _():
        for which in range(2):
            for copy in (own_to_across, next_to_across, across_to_next, far_to_next):
                for c in range(CHUNKS):
                    copy(which, c).wait_send()

    for j in range(LAYERS):
        part_copy(j).wait_send()

        @pl.loop(1, team)
        def _(i):
            ret_copy(j, i).wait_send()

    for j in (NEXT, ACROSS, FAR):
        for n in range(PARTS):
            sum_copy(j, n).wait_send()

    for copy in tables:
        copy.wait_send()
    halo.wait_send()

    @pl.loop(1, crew)
    def _(j):
        mix_copy(j).wait_send()
        mix_copy(j).wait_recv()

    mix_out[...] = mix[...]
    for store in stores:
        store.wait()


def expert_pass(
    stream, out_grad, ids, weights, gate_in, conv_gate, conv_value, taps, w_gate, w_up, w_down
):
    toks, width = stream.shape
    chans = gate_in.shape[1]
    count = lax.axis_size("sp")
    cap = 4 * toks // count
    team = count // LAYERS
    slots = team * cap
    tall = LAYERS * slots
    deep, hid = w_gate.shape[1:]
    crew = team_size(count)
    vmem = pl.BlockSpec(memory_space=pltpu.VMEM)
    anywhere = pl.BlockSpec(memory_space=pl.ANY)
    dma = pltpu.SemaphoreType.DMA
    return pl.pallas_call(
        functools.partial(expert_kernel, count, cap),
        out_shape=(
            jax.ShapeDtypeStruct((toks, width), BF16),
            jax.ShapeDtypeStruct((toks, chans), F32),
            jax.ShapeDtypeStruct((crew * toks, chans), BF16),
            jax.ShapeDtypeStruct((1, deep, hid), BF16),
            jax.ShapeDtypeStruct((1, deep, hid), BF16),
            jax.ShapeDtypeStruct((1, hid, deep), BF16),
        ),
        in_specs=[vmem] * 8 + [anywhere] * 3,
        out_specs=(vmem, vmem, vmem, anywhere, anywhere, anywhere),
        scratch_shapes=[
            pltpu.VMEM((2, LAYERS - 1, toks, width), BF16),
            pltpu.VMEM((LAYERS, 8, toks), F32),
            pltpu.VMEM((LAYERS, slots, toks), BF16),
            pltpu.VMEM((LAYERS, slots, 1), F32),
            pltpu.VMEM((2, LAYERS, slots, width), BF16),
            pltpu.VMEM((2, tall, width), BF16),
            pltpu.VMEM((2, tall, width), BF16),
            pltpu.VMEM((deep, hid), BF16),
            pltpu.VMEM((deep, hid), BF16),
            pltpu.VMEM((hid, deep), BF16),
            pltpu.VMEM((tall, hid), F32),
            pltpu.VMEM((tall, hid), F32),
            pltpu.VMEM((tall, hid), BF16),
            pltpu.VMEM((tall, hid), BF16),
            pltpu.VMEM((tall, hid), BF16),
            pltpu.VMEM((tall, width), BF16),
            pltpu.VMEM((tall, width), BF16),
            pltpu.VMEM((tall, width), BF16),
            pltpu.VMEM((tall, width), BF16),
            pltpu.VMEM((LAYERS - 1, toks, width), BF16),
            pltpu.VMEM((5, toks, width), BF16),
            pltpu.VMEM((toks, width), F32),
            pltpu.VMEM((deep, hid), BF16),
            pltpu.VMEM((deep, hid), BF16),
            pltpu.VMEM((hid, deep), BF16),
            pltpu.VMEM((crew * toks, chans), BF16),
            pltpu.VMEM((toks, chans), BF16),
            pltpu.VMEM((toks + 8, chans), F32),
            pltpu.VMEM((8, chans), F32),
            pltpu.VMEM((8, chans), F32),
            dma((3,)),
            dma((3,)),
            dma((2, 5, CHUNKS)),
            dma((2, LAYERS - 1, CHUNKS)),
            dma((3,)),
            dma((LAYERS,)),
            dma((2, LAYERS, team)),
            dma((2, LAYERS, team)),
            dma((2, LAYERS, team)),
            dma((2, LAYERS, team)),
            dma((LAYERS,)),
            dma((LAYERS,)),
            dma((LAYERS, team)),
            dma((LAYERS, team)),
            dma((LAYERS - 1, PARTS)),
            dma((5, PARTS)),
            dma((crew,)),
            dma((crew,)),
            dma((2,)),
        ],
        compiler_params=pltpu.CompilerParams(
            collective_id=0, has_side_effects=True, vmem_limit_bytes=62 * 1024 * 1024
        ),
    )(stream, out_grad, ids, weights, gate_in, conv_gate, conv_value, taps, w_gate, w_up, w_down)


def mixer_kernel(
    count,
    sh,
    w_out_hbm,
    mix,
    gate_in,
    wog_out,
    mg_out,
    halo_out,
    far,
    w_out,
    sg,
    p_send,
    p_recv,
    h_send,
    h_recv,
    w_sem,
    whole_sem,
    gsend_sem,
    grecv_sem,
    fsend_sem,
    frecv_sem,
    own_sem,
    psend_sem,
    precv_sem,
    hsem,
):
    me = lax.axis_index("sp")
    half = lax.axis_index("tp")
    other = 1 - half
    team = team_size(count)
    layers = count // team
    place, layer = lax.rem(me, team), me // team
    toks, width = sh.shape
    per = layers // 2
    blk = width // (team * per)
    load = pltpu.make_async_copy(w_out_hbm, w_out, w_sem)
    load.start()

    def member(j):
        return me - place + lax.rem(place + j, team)

    def floor(i):
        return lax.rem(layer + i, layers) * team + place

    after, before = lax.rem(me + 1, count), lax.rem(me + count - 1, count)
    barrier = pltpu.get_barrier_semaphore()

    def greet(device):
        pl.semaphore_signal(barrier, inc=1, device_id=device, device_id_type=MESH)

    for j in range(1, team):
        greet((member(j), half))
    for i in range(1, layers):
        greet((floor(i), half))
    greet((me, other))
    greet((after, half))
    greet((before, half))
    pl.semaphore_wait(barrier, team - 1 + layers - 1 + 3)

    def remote(src, dst, send, recv, device):
        return pltpu.make_async_remote_copy(
            src_ref=src,
            dst_ref=dst,
            send_sem=send,
            recv_sem=recv,
            device_id=device,
            device_id_type=MESH,
        )

    def cols(j, m):
        at = (lax.rem(place + j, team) + team * m) * blk
        return pl.ds(pl.multiple_of(at, blk), blk)

    def spot(h, m, size):
        return pl.ds(pl.multiple_of((h * per + m) * blk, blk), size)

    def stripe(j):
        return pl.ds(j * toks, toks)

    def piece(j, m):
        return remote(
            sh.at[:, cols(j, m)],
            sg.at[stripe(j), spot(half, m, blk)],
            gsend_sem.at[j, m],
            grecv_sem.at[j, m],
            (member(j), half),
        )

    def own_piece(m):
        return remote(
            sh.at[:, cols(0, m)],
            sg.at[stripe(0), spot(half, m, blk)],
            own_sem.at[0, m],
            own_sem.at[1, m],
            (me, other),
        )

    def handed(j):
        ref = sg.at[stripe(j), spot(half, 0, per * blk)]
        return remote(ref, ref, fsend_sem.at[j], frecv_sem.at[j], (me, other))

    whole = remote(sh, far, whole_sem.at[0], whole_sem.at[1], (me, other))
    whole.start()
    for j in range(1, team):
        for m in range(per):
            piece(j, m).start()
    for m in range(per):
        own_piece(m).start()
        sg[stripe(0), spot(half, m, blk)] = sh[:, cols(0, m)]

    load.wait()
    near_at = pl.ds(pl.multiple_of(half * width, width), width)
    far_at = pl.ds(pl.multiple_of(other * width, width), width)
    grad = dot(sh[...], w_out[near_at], 1, 0)
    whole.wait_recv()
    grad = (grad + dot(far[...], w_out[far_at], 1, 0)).astype(BF16)
    mg_out[...] = grad
    h_send[...] = grad[:8].astype(F32) * gate_in[:8].astype(F32)
    halo = remote(h_send, h_recv, hsem.at[0], hsem.at[1], (before, half))
    halo.start()
    for j in range(1, team):
        for m in range(per):
            piece(j, m).wait_recv()
        handed(j).start()
    for m in range(per):
        own_piece(m).wait_recv()
    for j in range(1, team):
        handed(j).wait_recv()

    def share(i):
        at = pl.ds(pl.multiple_of(lax.rem(layer + i, layers) * blk, blk), blk)
        return dot(sg[:, at].T, mix[...], 1, 0)

    def part(i):
        return remote(
            p_send.at[i], p_recv.at[i], psend_sem.at[i], precv_sem.at[i], (floor(i), half)
        )

    @pl.loop(1, layers)
    def _(i):
        p_send[i] = share(i).astype(BF16)
        part(i).start()

    wog_out[...] = share(0)
    for m in range(per):
        own_piece(m).wait_send()
    whole.wait_send()
    for j in range(1, team):
        for m in range(per):
            piece(j, m).wait_send()
        handed(j).wait_send()
    halo.wait_send()
    halo.wait_recv()
    halo_out[...] = h_recv[...]

    @pl.loop(1, layers)
    def _(i):
        part(i).wait_recv()
        wog_out[...] += p_recv[i].astype(F32)

    @pl.loop(1, layers)
    def _(i):
        part(i).wait_send()


def mixer_pass(stream_half, w_out, mix, gate_in):
    count = lax.axis_size("sp")
    team = team_size(count)
    layers = count // team
    per = layers // 2
    toks, width = stream_half.shape
    deep, chans = w_out.shape
    blk = deep // count
    vmem = pl.BlockSpec(memory_space=pltpu.VMEM)
    dma = pltpu.SemaphoreType.DMA
    return pl.pallas_call(
        functools.partial(mixer_kernel, count),
        out_shape=(
            jax.ShapeDtypeStruct((blk, chans), F32),
            jax.ShapeDtypeStruct((toks, chans), BF16),
            jax.ShapeDtypeStruct((8, chans), F32),
        ),
        in_specs=[vmem, pl.BlockSpec(memory_space=pl.ANY), vmem, vmem],
        out_specs=(vmem, vmem, vmem),
        scratch_shapes=[
            pltpu.VMEM((toks, width), BF16),
            pltpu.VMEM((deep, chans), BF16),
            pltpu.VMEM((team * toks, layers * blk), BF16),
            pltpu.VMEM((layers, blk, chans), BF16),
            pltpu.VMEM((layers, blk, chans), BF16),
            pltpu.VMEM((8, chans), F32),
            pltpu.VMEM((8, chans), F32),
            dma,
            dma((2,)),
            dma((team, per)),
            dma((team, per)),
            dma((team,)),
            dma((team,)),
            dma((2, per)),
            dma((layers,)),
            dma((layers,)),
            dma((2,)),
        ],
        compiler_params=pltpu.CompilerParams(
            collective_id=1, has_side_effects=True, vmem_limit_bytes=32 * 1024 * 1024
        ),
    )(stream_half, w_out, mix, gate_in)


def shards(
    stream,
    out_grad,
    gate_in,
    conv_gate,
    conv_value,
    taps,
    w_out,
    route_ids,
    route_weights,
    w_gate,
    w_up,
    w_down,
):
    tok_rows = stream.shape[0]
    me = lax.axis_index("sp")
    depth = taps.shape[0]
    channels = conv_gate.shape[1]
    stream_half, conv_sum, mix, gate_w_grad, up_w_grad, down_w_grad = expert_pass(
        stream,
        out_grad,
        route_ids.T,
        route_weights.T,
        gate_in,
        conv_gate,
        conv_value,
        taps,
        w_gate,
        w_up,
        w_down,
    )
    if w_out.shape[0] // lax.axis_size("sp") % 128 == 0:
        out_proj_grad, mixer_grad, halo = mixer_pass(stream_half, w_out, mix, gate_in)
    else:
        stream_whole = lax.all_gather(stream_half, "tp", axis=1, tiled=True)
        mixer_grad = dot(stream_whole, w_out, 1, 0).astype(BF16)
        out_proj_grad = lax.psum_scatter(
            dot(stream_whole, mix[:tok_rows], 0, 0).astype(BF16), "sp", scatter_dimension=0, tiled=True
        ).astype(F32)
        first = mixer_grad[: depth - 1].astype(F32) * gate_in[: depth - 1].astype(F32)
        halo = passed_along(first, "sp", -1)
    mixer_wide = mixer_grad.astype(jnp.float32)
    gate_in_grad = (mixer_wide * conv_sum).astype(jnp.bfloat16)
    conv_inner = mixer_wide * gate_in.astype(jnp.float32)
    right_rows = jnp.where(me == lax.axis_size("sp") - 1, 0.0, halo[: depth - 1])
    padded_back = jnp.concatenate([conv_inner, right_rows], axis=0)
    prod_grad = jnp.zeros((tok_rows, channels), jnp.float32)
    for tap_index in range(depth):
        offset = depth - 1 - tap_index
        prod_grad = prod_grad + taps[tap_index][None, :] * padded_back[offset : offset + tok_rows]
    conv_gate_grad = (prod_grad * conv_value.astype(jnp.float32)).astype(jnp.bfloat16)
    conv_value_grad = (prod_grad * conv_gate.astype(jnp.float32)).astype(jnp.bfloat16)
    return (
        stream_half,
        gate_in_grad,
        conv_gate_grad,
        conv_value_grad,
        out_proj_grad,
        gate_w_grad.astype(F32),
        up_w_grad.astype(F32),
        down_w_grad.astype(F32),
    )


def solution(mesh):
    placed = (
        P("sp", "tp"),
        P("sp", "tp"),
        P("sp", "tp"),
        P("sp", "tp"),
        P("sp", "tp"),
        P(None, "tp"),
        P(None, "tp"),
        P("sp", None),
        P("sp", None),
        P("sp", None, "tp"),
        P("sp", None, "tp"),
        P("sp", "tp", None),
    )
    return jax.shard_map(
        shards,
        mesh=mesh,
        in_specs=placed,
        out_specs=(
            P("sp", "tp"),
            P("sp", "tp"),
            P("sp", "tp"),
            P("sp", "tp"),
            P("sp", "tp"),
            P("sp", None, "tp"),
            P("sp", None, "tp"),
            P("sp", "tp", None),
        ),
        check_vma=False,
    )
```

```python
import functools

import jax
import jax.numpy as jnp
from jax import lax
from jax.experimental import pallas as pl
from jax.experimental.pallas import tpu as pltpu
from jax.sharding import PartitionSpec as P

MESH = pl.DeviceIdType.MESH
LAYERS = 4
PARTS = 4
CHUNKS = 4
F32 = jnp.float32
BF16 = jnp.bfloat16
OWN, NEXT, ACROSS, FAR = 0, 1, 2, 3


def passed_along(shard, axis, by):
    count = lax.axis_size(axis)
    pairs = [(i, i + by) for i in range(count) if 0 <= i + by < count]
    return lax.ppermute(shard, axis, pairs)


def dot(a, b, ca, cb):
    return lax.dot_general(a, b, (((ca,), (cb,)), ((), ())), preferred_element_type=F32)


def expert_kernel(
    count,
    cap,
    fused,
    stream_in,
    grad_in,
    ids,
    weights,
    gate_in,
    conv_gate,
    conv_value,
    taps,
    wg_hbm,
    wu_hbm,
    wd_hbm,
    wo_hbm,
    half_out,
    gate_out,
    up_out,
    down_out,
    first_out,
    second_out,
    third_out,
    fourth_out,
    toks_in,
    table,
    pick,
    scale,
    rel,
    rows,
    cot,
    wg,
    wu,
    wd,
    pre_g,
    pre_u,
    hidden,
    gg,
    ug,
    part_out,
    part_in,
    ret,
    back,
    col_out,
    col_in,
    total,
    gate_f,
    up_f,
    down_f,
    mix,
    mix_src,
    padded,
    conv_sum,
    halo_src,
    halo_dst,
    wo,
    far_half,
    strips,
    share_out,
    share_in,
    edge_src,
    edge_dst,
    w_sem,
    out_sem,
    z_send,
    z_recv,
    t_send,
    t_recv,
    i_send,
    i_recv,
    f_send,
    f_recv,
    p_send,
    p_recv,
    r_send,
    r_recv,
    c_send,
    c_recv,
    m_send,
    m_recv,
    h_sem,
    g_send,
    g_recv,
    own_sem,
    d_send,
    d_recv,
    s_send,
    s_recv,
    b_send,
    b_recv,
    e_sem,
):
    me = lax.axis_index("sp")
    half = lax.axis_index("tp")
    other = 1 - half
    team = count // LAYERS
    place, layer = lax.rem(me, team), me // team
    side = layer // 2
    inner = lax.rem(layer + 1, LAYERS) >= 2
    outer = jnp.logical_not(inner)
    next_layer = layer + 1 - 2 * lax.rem(layer, 2)
    across_layer = 2 - side
    far_layer = 3 * (1 - side)
    toks, width = stream_in.shape
    slots = team * cap
    depth = taps.shape[0]
    top = ids.shape[0]

    def column(at):
        return (at * team + place, half)

    def teammate(i):
        return layer * team + lax.rem(place + i, team)

    loads = []
    for n, (a, b) in enumerate(((wg_hbm, wg), (wu_hbm, wu), (wd_hbm, wd))):
        load = pltpu.make_async_copy(a.at[0], b, w_sem.at[n])
        load.start()
        loads.append(load)
    if fused:
        load = pltpu.make_async_copy(wo_hbm, wo, w_sem.at[3])
        load.start()
        loads.append(load)

    after, before = lax.rem(me + 1, count), lax.rem(me + count - 1, count)
    barrier = pltpu.get_barrier_semaphore()

    def greet(device):
        pl.semaphore_signal(barrier, inc=1, device_id=device, device_id_type=MESH)

    greet(column(lax.rem(layer + 1, LAYERS)))
    greet(column(lax.rem(layer + 2, LAYERS)))
    greet(column(lax.rem(layer + 3, LAYERS)))

    @pl.loop(1, team)
    def _(i):
        greet((teammate(i), half))

    greet((me, other))
    greet((after, half))
    greet((before, half))
    pl.semaphore_wait(barrier, LAYERS - 1 + team - 1 + 3)

    def remote(src, dst, send, recv, device):
        return pltpu.make_async_remote_copy(
            src_ref=src,
            dst_ref=dst,
            send_sem=send,
            recv_sem=recv,
            device_id=device,
            device_id_type=MESH,
        )

    def block(k):
        return pl.ds(pl.multiple_of(k * cap, cap), cap)

    def piece(j, k):
        return pl.ds(pl.multiple_of(j * slots + k * cap, cap), cap)

    def group(j):
        return pl.ds(j * slots, slots)

    whole = (stream_in, grad_in)

    def blocks_of(which, j):
        return whole[which] if j == OWN else toks_in.at[which, j - 1]

    stretch = toks // CHUNKS

    def hop(which, n, j, to, lands, c):
        at = pl.ds(c * stretch, stretch)
        return remote(
            blocks_of(which, j).at[at],
            toks_in.at[which, lands - 1, at],
            z_send.at[which, n, c],
            z_recv.at[which, lands - 1, c],
            column(to),
        )

    def own_to_next(which, c):
        return hop(which, 0, OWN, next_layer, NEXT, c)

    def own_to_across(which, c):
        return hop(which, 1, OWN, across_layer, ACROSS, c)

    def next_to_across(which, c):
        return hop(which, 2, NEXT, across_layer, FAR, c)

    def across_to_next(which, c):
        return hop(which, 3, ACROSS, next_layer, ACROSS, c)

    def far_to_next(which, c):
        return hop(which, 4, FAR, next_layer, FAR, c)

    def arrived(which, j):
        for c in range(CHUNKS):
            hop(which, 0, j, next_layer, j, c).wait_recv()

    def begin(copy, which):
        for c in range(CHUNKS):
            copy(which, c).start()

    def relay(*steps):
        for c in range(CHUNKS):
            for which, j, copy in steps:
                hop(which, 0, j, next_layer, j, c).wait_recv()
                copy(which, c).start()

    last = pl.ds(toks - 8, 8)
    halo_src[...] = conv_gate[last].astype(F32) * conv_value[last].astype(F32)
    halo = remote(halo_src, halo_dst, h_sem.at[0], h_sem.at[1], (after, half))
    halo.start()
    begin(own_to_next, 0)

    @pl.when(inner)
    def _():
        begin(own_to_across, 0)

    expert = lax.broadcasted_iota(jnp.int32, (count, toks), 0)
    hits = [ids[k : k + 1] == expert for k in range(top)]
    named = functools.reduce(jnp.logical_or, hits)
    named = jnp.where(named, 1.0, 0.0).astype(BF16)
    early = lax.broadcasted_iota(jnp.int32, (toks, toks), 0)
    late = lax.broadcasted_iota(jnp.int32, (toks, toks), 1)
    earlier = jnp.where(early < late, 1.0, 0.0).astype(BF16)
    spots = dot(named, earlier, 1, 0) + (expert * cap).astype(F32)
    table[OWN] = jnp.zeros(table.shape[1:], F32)
    for k in range(top):
        table[OWN, k : k + 1] = jnp.sum(jnp.where(hits[k], spots, 0.0), axis=0, keepdims=True)
        table[OWN, top + k : top + k + 1] = weights[k : k + 1]

    seen_as = jnp.where(inner, ACROSS, FAR)

    def table_copy(n, to, lands):
        return remote(
            table.at[OWN], table.at[lands], t_send.at[n], t_recv.at[lands], column(to)
        )

    tables = (
        table_copy(0, next_layer, NEXT),
        table_copy(1, across_layer, seen_as),
        table_copy(2, far_layer, seen_as),
    )
    for copy in tables:
        copy.start()

    begin(own_to_next, 1)

    base = (layer * slots).astype(F32)

    def choose(j):
        spot = lax.broadcasted_iota(jnp.int32, (slots, toks), 0).astype(F32)
        found = [table[j, k : k + 1] - base == spot for k in range(top)]
        pick[j] = jnp.where(functools.reduce(jnp.logical_or, found), 1.0, 0.0).astype(BF16)
        scale[j] = sum(
            jnp.sum(
                jnp.where(found[k], table[j, top + k : top + k + 1], 0.0), axis=1, keepdims=True
            )
            for k in range(top)
        )

    bufs = (rows, cot)

    def in_copy(which, j, i):
        return remote(
            rel.at[which, j, block(lax.rem(place + i, team))],
            bufs[which].at[half, piece(j, place)],
            i_send.at[which, j, i],
            i_recv.at[which, j, i],
            (teammate(i), half),
        )

    def in_arrival(which, j, i):
        at = bufs[which].at[half, piece(j, lax.rem(place - i + team, team))]
        return remote(at, at, i_send.at[which, j, i], i_recv.at[which, j, i], (teammate(i), half))

    def pass_copy(which, j, i):
        at = bufs[which].at[half, piece(j, lax.rem(place - i + team, team))]
        return remote(at, at, f_send.at[which, j, i], f_recv.at[which, j, i], (me, other))

    def own_pass(which, j):
        return remote(
            rel.at[which, j, block(place)],
            bufs[which].at[half, piece(j, place)],
            f_send.at[which, j, 0],
            f_recv.at[which, j, 0],
            (me, other),
        )

    def deal(which, j):
        chosen = dot(pick[j], blocks_of(which, j)[...], 1, 0)
        if which == 1:
            chosen = scale[j] * chosen
        rel[which, j] = chosen.astype(BF16)

        @pl.loop(1, team)
        def _(i):
            in_copy(which, j, i).start()

        own_pass(which, j).start()
        bufs[which][half, piece(j, place)] = rel[which, j, block(place)]

    def gather(which, j):
        @pl.loop(1, team)
        def _(i):
            in_arrival(which, j, i).wait_recv()
            pass_copy(which, j, i).start()

        @pl.loop(0, team)
        def _(i):
            pass_copy(which, j, i).wait_recv()

    mine_at = pl.ds(pl.multiple_of(half * width, width), width)
    other_at = pl.ds(pl.multiple_of(other * width, width), width)

    def part_copy(j):
        return remote(
            part_out.at[group(j)], part_in.at[group(j)], p_send.at[j], p_recv.at[j], (me, other)
        )

    def ret_copy(j, i):
        return remote(
            ret.at[piece(j, lax.rem(place + i, team))],
            back.at[piece(j, place)],
            r_send.at[j, i],
            r_recv.at[j, i],
            (teammate(i), half),
        )

    def ret_arrival(j, i):
        at = back.at[piece(j, lax.rem(place - i + team, team))]
        return remote(at, at, r_send.at[j, i], r_recv.at[j, i], (teammate(i), half))

    def ahead(j):
        gather(0, j)
        at = group(j)
        left, right = rows[0, at], rows[1, at]
        pre_g[at] = dot(left, wg[:width], 1, 0) + dot(right, wg[width:], 1, 0)
        pre_u[at] = dot(left, wu[:width], 1, 0) + dot(right, wu[width:], 1, 0)

    def behind(j):
        gather(1, j)
        at = group(j)
        grad = dot(cot[0, at], wd[:, :width], 1, 1) + dot(cot[1, at], wd[:, width:], 1, 1)
        pg, pu = pre_g[at], pre_u[at]
        sig = jax.nn.sigmoid(pg)
        silu = pg * sig
        hidden[at] = (silu * pu).astype(BF16)
        ug_now = (grad * silu).astype(BF16)
        gg_now = (grad * pu * sig * (1.0 + pg * (1.0 - sig))).astype(BF16)
        ug[at] = ug_now
        gg[at] = gg_now
        far = dot(gg_now, wg[other_at], 1, 1) + dot(ug_now, wu[other_at], 1, 1)
        part_out[at] = far.astype(BF16)
        part_copy(j).start()
        near = dot(gg_now, wg[mine_at], 1, 1) + dot(ug_now, wu[mine_at], 1, 1)
        near = near.astype(BF16).astype(F32)
        part_copy(j).wait_recv()
        ret[at] = (near + part_in[at].astype(F32)).astype(BF16)

        @pl.loop(1, team)
        def _(i):
            ret_copy(j, i).start()

        back[piece(j, place)] = ret[piece(j, place)]

    def returned(j):
        @pl.loop(1, team)
        def _(i):
            ret_arrival(j, i).wait_recv()

    share = width // PARTS

    def cols(n):
        return pl.ds(n * share, share)

    def sum_copy(j, n):
        if j == NEXT:
            to, lands = next_layer, 0
        else:
            to = jnp.where(inner, across_layer, next_layer)
            lands = jnp.where(inner, j - 1, j + 1)
        return remote(
            col_out.at[j - 1, :, cols(n)],
            col_in.at[lands, :, cols(n)],
            c_send.at[j - 1, n],
            c_recv.at[lands, n],
            column(to),
        )

    def sum_arrival(lands, n):
        at = col_in.at[lands, :, cols(n)]
        return remote(at, at, c_send.at[0, n], c_recv.at[lands, n], column(next_layer))

    def partial(j, n):
        return dot(pick[j], back[group(j), cols(n)], 0, 0)

    def send_sums(j):
        for n in range(PARTS):
            col_out[j - 1, :, cols(n)] = partial(j, n).astype(BF16)
            sum_copy(j, n).start()

    def forward_sum(j, n):
        mine = partial(j, n)
        sum_arrival(j + 1, n).wait_recv()
        mine = mine + col_in[j + 1, :, cols(n)].astype(F32)
        col_out[j - 1, :, cols(n)] = mine.astype(BF16)
        sum_copy(j, n).start()

    choose(OWN)
    deal(0, OWN)
    deal(1, OWN)

    halo.wait_recv()
    prod = conv_gate[...].astype(F32) * conv_value[...].astype(F32)
    padded[8:] = prod
    padded[:8] = jnp.where(me == 0, 0.0, halo_dst[...])
    conv = jnp.zeros(prod.shape, F32)
    for tap in range(depth):
        start = 8 - (depth - 1) + tap
        conv = conv + taps[tap : tap + 1] * padded[start : start + toks]
    conv_sum[...] = conv
    mix_src[...] = (gate_in[...].astype(F32) * conv).astype(BF16)

    def mix_copy(j):
        return remote(
            mix_src,
            mix.at[pl.ds(pl.multiple_of(j * toks, toks), toks)],
            m_send.at[j],
            m_recv.at[j],
            (teammate(j), half),
        )

    def informed(j):
        table_copy(0, next_layer, j).wait_recv()
        choose(j)

    @pl.when(inner)
    def _():
        relay((0, NEXT, next_to_across), (0, ACROSS, across_to_next))

    @pl.when(outer)
    def _():
        arrived(0, NEXT)

    informed(NEXT)
    deal(0, NEXT)
    for load in loads:
        load.wait()

    @pl.when(inner)
    def _():
        relay((1, NEXT, next_to_across), (0, FAR, far_to_next))
        begin(own_to_across, 1)

    @pl.when(outer)
    def _():
        arrived(1, NEXT)

    deal(1, NEXT)
    ahead(OWN)
    behind(OWN)

    @pl.when(inner)
    def _():
        relay((1, FAR, far_to_next))

    ahead(NEXT)
    behind(NEXT)

    @pl.when(outer)
    def _():
        arrived(0, ACROSS)

    informed(ACROSS)
    deal(0, ACROSS)
    returned(OWN)
    total[...] = dot(pick[OWN], back[group(OWN)], 0, 0)
    returned(NEXT)

    @pl.when(outer)
    def _():
        send_sums(NEXT)
        arrived(0, FAR)

    informed(FAR)
    deal(0, FAR)

    @pl.when(inner)
    def _():
        relay((1, ACROSS, across_to_next))

    ahead(ACROSS)

    @pl.when(outer)
    def _():
        arrived(1, FAR)

    deal(1, FAR)
    ahead(FAR)

    @pl.when(outer)
    def _():
        arrived(1, ACROSS)

    deal(1, ACROSS)
    behind(FAR)
    behind(ACROSS)

    if fused:

        @pl.loop(1, team)
        def _(j):
            mix_copy(j).start()

        mix[pl.ds(0, toks)] = mix_src[...]

    returned(FAR)

    @pl.when(outer)
    def _():
        send_sums(FAR)

    hid_part = hidden.shape[1] // PARTS
    deep_part = width // PARTS

    def weights_part(n):
        to = pl.ds(n * hid_part, hid_part)
        x = hidden[:, to].T
        for h in range(2):
            down_f[to, h * width : (h + 1) * width] = dot(x, cot[h], 1, 0).astype(BF16)

        @pl.loop(0, 2)
        def _(h):
            to = pl.ds(pl.multiple_of(h * width + n * deep_part, deep_part), deep_part)
            x = rows[h, :, n * deep_part : (n + 1) * deep_part].T
            gate_f[to] = dot(x, gg[...], 1, 0).astype(BF16)
            up_f[to] = dot(x, ug[...], 1, 0).astype(BF16)

    for n in range(PARTS):

        @pl.when(inner)
        def _():
            forward_sum(FAR, n)

        weights_part(n)

    stores = [
        pltpu.make_async_copy(gate_f, gate_out.at[0], out_sem.at[0]),
        pltpu.make_async_copy(up_f, up_out.at[0], out_sem.at[1]),
        pltpu.make_async_copy(down_f, down_out.at[0], out_sem.at[2]),
    ]
    for store in stores:
        store.start()

    returned(ACROSS)

    @pl.when(outer)
    def _():
        send_sums(ACROSS)

    @pl.when(inner)
    def _():
        for n in range(PARTS):
            forward_sum(NEXT, n)
            forward_sum(ACROSS, n)

        for n in range(PARTS):
            sum_arrival(1, n).wait_recv()
            total[:, cols(n)] += col_in[1, :, cols(n)].astype(F32)

    per = LAYERS // 2
    blk = width // (team * per)

    def band(b):
        return pl.ds(b * blk, blk)

    def spot(h, m, size):
        return pl.ds(pl.multiple_of((h * per + m) * blk, blk), size)

    def stripe(j):
        return pl.ds(pl.multiple_of(j * toks, toks), toks)

    def piece_copy(b, j, m):
        return remote(
            half_out.at[:, band(b)],
            strips.at[stripe(j), spot(half, m, blk)],
            g_send.at[j, m],
            g_recv.at[j, m],
            (teammate(j), half),
        )

    def own_piece(b, m):
        return remote(
            half_out.at[:, band(b)],
            strips.at[stripe(0), spot(half, m, blk)],
            own_sem.at[0, m],
            own_sem.at[1, m],
            (me, other),
        )

    def whole_copy(n):
        return remote(
            half_out.at[:, cols(n)], far_half.at[:, cols(n)], b_send.at[n], b_recv.at[n], (me, other)
        )

    def handed(j):
        at = strips.at[stripe(j), spot(half, 0, per * blk)]
        return remote(at, at, d_send.at[j], d_recv.at[j], (me, other))

    def layer_copy(i):
        to = lax.rem(layer + i, LAYERS)
        return remote(share_out.at[i], share_in.at[i], s_send.at[i], s_recv.at[i], column(to))

    def settle(n):
        sum_arrival(0, n).wait_recv()
        now = total[:, cols(n)] + col_in[0, :, cols(n)].astype(F32)
        half_out[:, cols(n)] = (grad_in[:, cols(n)].astype(F32) + now).astype(BF16)
        if fused:
            whole_copy(n).start()
            for b in range(n * share // blk, (n + 1) * share // blk):
                j, m = lax.rem(b % team - place + team, team), b // team

                @pl.when(j > 0)
                def _():
                    piece_copy(b, j, m).start()

                @pl.when(j == 0)
                def _():
                    own_piece(b, m).start()
                    strips[stripe(0), spot(half, m, blk)] = half_out[:, band(b)]

    def edge_copy():
        return remote(edge_src, edge_dst, e_sem.at[0], e_sem.at[1], (before, half))

    def mixer_grad():
        mixed = dot(half_out[...], wo[mine_at], 1, 0)
        for n in range(PARTS):
            whole_copy(n).wait_recv()
        mixed = (mixed + dot(far_half[...], wo[other_at], 1, 0)).astype(BF16)
        wide = mixed.astype(F32)
        inner_conv = wide * gate_in[...].astype(F32)
        edge_src[...] = inner_conv[:8]
        edge_copy().start()
        padded[:toks] = inner_conv
        second_out[...] = (wide * conv_sum[...]).astype(BF16)

    def conv_grads():
        edge_copy().wait_recv()
        padded[toks:] = jnp.where(me == count - 1, 0.0, edge_dst[...])
        prod_grad = jnp.zeros((toks, taps.shape[1]), F32)
        for tap in range(depth):
            start = depth - 1 - tap
            prod_grad = prod_grad + taps[tap : tap + 1] * padded[start : start + toks]
        third_out[...] = (prod_grad * conv_value[...].astype(F32)).astype(BF16)
        fourth_out[...] = (prod_grad * conv_gate[...].astype(F32)).astype(BF16)

    def strips_in():
        @pl.loop(1, team)
        def _(j):
            for m in range(per):
                piece_copy(0, j, m).wait_recv()
            handed(j).start()

        for m in range(per):
            own_piece(0, m).wait_recv()

        @pl.loop(1, team)
        def _(j):
            handed(j).wait_recv()
            mix_copy(j).wait_recv()

    def layer_share(i):
        at = pl.ds(pl.multiple_of(lax.rem(layer + i, LAYERS) * blk, blk), blk)
        return dot(strips[:, at].T, mix[...], 1, 0)

    def shares_out():
        for i in (2, 1, 3):
            share_out[i] = layer_share(i).astype(BF16)
            layer_copy(i).start()
        first_out[...] = layer_share(0)

    def shares_in():
        for i in (1, 3, 2):
            layer_copy(i).wait_recv()
            first_out[...] += share_in[i].astype(F32)

    for n in range(PARTS):
        settle(n)
    if fused:
        strips_in()
        shares_out()
        mixer_grad()
        conv_grads()
        shares_in()
    else:
        first_out[...] = conv_sum[...]
        second_out[...] = mix_src[...]
        fourth_out[...] = jnp.zeros(fourth_out.shape, fourth_out.dtype)
        third_out[...] = jnp.zeros(third_out.shape, third_out.dtype)

    for which in range(2):
        for c in range(CHUNKS):
            own_to_next(which, c).wait_send()

        for j in range(LAYERS):
            own_pass(which, j).wait_send()

            @pl.loop(1, team)
            def _(i):
                in_copy(which, j, i).wait_send()
                pass_copy(which, j, i).wait_send()

    @pl.when(inner)
    def _():
        for which in range(2):
            for copy in (own_to_across, next_to_across, across_to_next, far_to_next):
                for c in range(CHUNKS):
                    copy(which, c).wait_send()

    for j in range(LAYERS):
        part_copy(j).wait_send()

        @pl.loop(1, team)
        def _(i):
            ret_copy(j, i).wait_send()

    for j in (NEXT, ACROSS, FAR):
        for n in range(PARTS):
            sum_copy(j, n).wait_send()

    for copy in tables:
        copy.wait_send()
    halo.wait_send()

    if fused:
        edge_copy().wait_send()
        for n in range(PARTS):
            whole_copy(n).wait_send()
        for m in range(per):
            own_piece(0, m).wait_send()

        @pl.loop(1, team)
        def _(j):
            mix_copy(j).wait_send()
            handed(j).wait_send()
            for m in range(per):
                piece_copy(0, j, m).wait_send()

        for i in range(1, LAYERS):
            layer_copy(i).wait_send()

    for store in stores:
        store.wait()


def expert_pass(
    fused,
    stream,
    out_grad,
    ids,
    weights,
    gate_in,
    conv_gate,
    conv_value,
    taps,
    w_gate,
    w_up,
    w_down,
    w_out,
):
    toks, width = stream.shape
    chans = gate_in.shape[1]
    count = lax.axis_size("sp")
    cap = 4 * toks // count
    team = count // LAYERS
    slots = team * cap
    tall = LAYERS * slots
    deep, hid = w_gate.shape[1:]
    blk = deep // count
    if fused:
        extra = (((blk, chans), F32),) + (((toks, chans), BF16),) * 3
    else:
        extra = (((toks, chans), F32), ((toks, chans), BF16)) + (((8, chans), F32),) * 2
    crew = team if fused else 1
    vmem = pl.BlockSpec(memory_space=pltpu.VMEM)
    anywhere = pl.BlockSpec(memory_space=pl.ANY)
    dma = pltpu.SemaphoreType.DMA
    return pl.pallas_call(
        functools.partial(expert_kernel, count, cap, fused),
        out_shape=(
            jax.ShapeDtypeStruct((toks, width), BF16),
            jax.ShapeDtypeStruct((1, deep, hid), BF16),
            jax.ShapeDtypeStruct((1, deep, hid), BF16),
            jax.ShapeDtypeStruct((1, hid, deep), BF16),
        )
        + tuple(jax.ShapeDtypeStruct(*one) for one in extra),
        in_specs=[vmem] * 8 + [anywhere] * 4,
        out_specs=(vmem,) + (anywhere,) * 3 + (vmem,) * 4,
        scratch_shapes=[
            pltpu.VMEM((2, LAYERS - 1, toks, width), BF16),
            pltpu.VMEM((LAYERS, 8, toks), F32),
            pltpu.VMEM((LAYERS, slots, toks), BF16),
            pltpu.VMEM((LAYERS, slots, 1), F32),
            pltpu.VMEM((2, LAYERS, slots, width), BF16),
            pltpu.VMEM((2, tall, width), BF16),
            pltpu.VMEM((2, tall, width), BF16),
            pltpu.VMEM((deep, hid), BF16),
            pltpu.VMEM((deep, hid), BF16),
            pltpu.VMEM((hid, deep), BF16),
            pltpu.VMEM((tall, hid), F32),
            pltpu.VMEM((tall, hid), F32),
            pltpu.VMEM((tall, hid), BF16),
            pltpu.VMEM((tall, hid), BF16),
            pltpu.VMEM((tall, hid), BF16),
            pltpu.VMEM((tall, width), BF16),
            pltpu.VMEM((tall, width), BF16),
            pltpu.VMEM((tall, width), BF16),
            pltpu.VMEM((tall, width), BF16),
            pltpu.VMEM((LAYERS - 1, toks, width), BF16),
            pltpu.VMEM((5, toks, width), BF16),
            pltpu.VMEM((toks, width), F32),
            pltpu.VMEM((deep, hid), BF16),
            pltpu.VMEM((deep, hid), BF16),
            pltpu.VMEM((hid, deep), BF16),
            pltpu.VMEM((crew * toks, chans), BF16),
            pltpu.VMEM((toks, chans), BF16),
            pltpu.VMEM((toks + 8, chans), F32),
            pltpu.VMEM((toks, chans), F32),
            pltpu.VMEM((8, chans), F32),
            pltpu.VMEM((8, chans), F32),
            pltpu.VMEM((deep, chans) if fused else (16, 128), BF16),
            pltpu.VMEM((toks, width) if fused else (16, 128), BF16),
            pltpu.VMEM((team * toks, LAYERS * blk) if fused else (16, 128), BF16),
            pltpu.VMEM((LAYERS, blk, chans), BF16),
            pltpu.VMEM((LAYERS, blk, chans), BF16),
            pltpu.VMEM((8, chans), F32),
            pltpu.VMEM((8, chans), F32),
            dma((4,)),
            dma((3,)),
            dma((2, 5, CHUNKS)),
            dma((2, LAYERS - 1, CHUNKS)),
            dma((3,)),
            dma((LAYERS,)),
            dma((2, LAYERS, team)),
            dma((2, LAYERS, team)),
            dma((2, LAYERS, team)),
            dma((2, LAYERS, team)),
            dma((LAYERS,)),
            dma((LAYERS,)),
            dma((LAYERS, team)),
            dma((LAYERS, team)),
            dma((LAYERS - 1, PARTS)),
            dma((5, PARTS)),
            dma((crew,)),
            dma((crew,)),
            dma((2,)),
            dma((team, LAYERS // 2)),
            dma((team, LAYERS // 2)),
            dma((2, LAYERS // 2)),
            dma((team,)),
            dma((team,)),
            dma((LAYERS,)),
            dma((LAYERS,)),
            dma((PARTS,)),
            dma((PARTS,)),
            dma((2,)),
        ],
        compiler_params=pltpu.CompilerParams(
            collective_id=0, has_side_effects=True, vmem_limit_bytes=62 * 1024 * 1024
        ),
    )(
        stream,
        out_grad,
        ids,
        weights,
        gate_in,
        conv_gate,
        conv_value,
        taps,
        w_gate,
        w_up,
        w_down,
        w_out,
    )


def publish_kernel(small, large, *refs):
    total = small + large
    ins, outs, refs = refs[:total], refs[total : 2 * total], refs[2 * total :]
    held, wide, (in_sem, out_sem) = refs[:total], refs[total : total + large], refs[total + large :]

    def spots(k):
        if k < small:
            return [(0, slice(None), slice(None))]
        size = held[k].shape[0] // PARTS
        return [(n, (0, pl.ds(n * size, size)), pl.ds(n * size, size)) for n in range(PARTS)]

    def load(k, n, outer_at, at):
        src = ins[k] if k < small else ins[k].at[outer_at]
        dst = held[k] if k < small else held[k].at[at]
        return pltpu.make_async_copy(src, dst, in_sem.at[k, n])

    def store(k, n, outer_at, at):
        src = held[k] if k < small else wide[k - small].at[at]
        dst = outs[k] if k < small else outs[k].at[outer_at]
        return pltpu.make_async_copy(src, dst, out_sem.at[k, n])

    order = list(range(small, total)) + list(range(small))
    steps = [(k, *spot) for k in order for spot in spots(k)]
    for step in steps:
        load(*step).start()
    for step in steps:
        load(*step).wait()
        k, at = step[0], step[3]
        if k >= small:
            wide[k - small][at] = held[k][at].astype(F32)
        store(*step).start()
    for step in steps:
        store(*step).wait()


def publish(smalls, larges):
    anywhere = pl.BlockSpec(memory_space=pl.ANY)
    dma = pltpu.SemaphoreType.DMA
    total = len(smalls) + len(larges)
    outs = [jax.ShapeDtypeStruct(x.shape, x.dtype) for x in smalls]
    outs += [jax.ShapeDtypeStruct(x.shape, F32) for x in larges]
    return pl.pallas_call(
        functools.partial(publish_kernel, len(smalls), len(larges)),
        out_shape=tuple(outs),
        in_specs=[anywhere] * total,
        out_specs=(anywhere,) * total,
        scratch_shapes=[pltpu.VMEM(x.shape, x.dtype) for x in smalls]
        + [pltpu.VMEM(x.shape[1:], BF16) for x in larges]
        + [pltpu.VMEM(x.shape[1:], F32) for x in larges]
        + [dma((total, PARTS)), dma((total, PARTS))],
        compiler_params=pltpu.CompilerParams(vmem_limit_bytes=62 * 1024 * 1024),
    )(*smalls, *larges)


def shards(
    stream,
    out_grad,
    gate_in,
    conv_gate,
    conv_value,
    taps,
    w_out,
    route_ids,
    route_weights,
    w_gate,
    w_up,
    w_down,
):
    tok_rows, channels = conv_gate.shape
    me = lax.axis_index("sp")
    depth = taps.shape[0]
    fused = w_out.shape[0] // lax.axis_size("sp") % 128 == 0
    stream_half, gate_w_grad, up_w_grad, down_w_grad, *extra = expert_pass(
        fused,
        stream,
        out_grad,
        route_ids.T,
        route_weights.T,
        gate_in,
        conv_gate,
        conv_value,
        taps,
        w_gate,
        w_up,
        w_down,
        w_out,
    )
    if fused:
        out_proj_grad, *chan_grads = extra
        smalls = (stream_half, *chan_grads, out_proj_grad)
        return publish(smalls, (gate_w_grad, up_w_grad, down_w_grad))
    conv_sum, mixer_out = extra[:2]
    stream_whole = lax.all_gather(stream_half, "tp", axis=1, tiled=True)
    mixer_grad = dot(stream_whole, w_out, 1, 0).astype(BF16)
    out_proj_grad = lax.psum_scatter(
        dot(stream_whole, mixer_out, 0, 0).astype(BF16), "sp", scatter_dimension=0, tiled=True
    ).astype(F32)
    first = mixer_grad[: depth - 1].astype(F32) * gate_in[: depth - 1].astype(F32)
    halo = passed_along(first, "sp", -1)
    mixer_wide = mixer_grad.astype(jnp.float32)
    gate_in_grad = (mixer_wide * conv_sum).astype(jnp.bfloat16)
    conv_inner = mixer_wide * gate_in.astype(jnp.float32)
    right_rows = jnp.where(me == lax.axis_size("sp") - 1, 0.0, halo[: depth - 1])
    padded_back = jnp.concatenate([conv_inner, right_rows], axis=0)
    prod_grad = jnp.zeros((tok_rows, channels), jnp.float32)
    for tap_index in range(depth):
        offset = depth - 1 - tap_index
        prod_grad = prod_grad + taps[tap_index][None, :] * padded_back[offset : offset + tok_rows]
    conv_gate_grad = (prod_grad * conv_value.astype(jnp.float32)).astype(jnp.bfloat16)
    conv_value_grad = (prod_grad * conv_gate.astype(jnp.float32)).astype(jnp.bfloat16)
    return (
        stream_half,
        gate_in_grad,
        conv_gate_grad,
        conv_value_grad,
        out_proj_grad,
        gate_w_grad.astype(F32),
        up_w_grad.astype(F32),
        down_w_grad.astype(F32),
    )


def solution(mesh):
    placed = (
        P("sp", "tp"),
        P("sp", "tp"),
        P("sp", "tp"),
        P("sp", "tp"),
        P("sp", "tp"),
        P(None, "tp"),
        P(None, "tp"),
        P("sp", None),
        P("sp", None),
        P("sp", None, "tp"),
        P("sp", None, "tp"),
        P("sp", "tp", None),
    )
    return jax.shard_map(
        shards,
        mesh=mesh,
        in_specs=placed,
        out_specs=(
            P("sp", "tp"),
            P("sp", "tp"),
            P("sp", "tp"),
            P("sp", "tp"),
            P("sp", "tp"),
            P("sp", None, "tp"),
            P("sp", None, "tp"),
            P("sp", "tp", None),
        ),
        check_vma=False,
    )
```

```python
import functools

import jax
import jax.numpy as jnp
from jax import lax
from jax.experimental import pallas as pl
from jax.experimental.pallas import tpu as pltpu
from jax.sharding import PartitionSpec as P

MESH = pl.DeviceIdType.MESH
LAYERS = 4
PARTS = 4
CHUNKS = 4
F32 = jnp.float32
BF16 = jnp.bfloat16
OWN, NEXT, ACROSS, FAR = 0, 1, 2, 3


def passed_along(shard, axis, by):
    count = lax.axis_size(axis)
    pairs = [(i, i + by) for i in range(count) if 0 <= i + by < count]
    return lax.ppermute(shard, axis, pairs)


def dot(a, b, ca, cb):
    return lax.dot_general(a, b, (((ca,), (cb,)), ((), ())), preferred_element_type=F32)


def expert_kernel(
    count,
    cap,
    fused,
    stream_hbm,
    grad_hbm,
    ids_hbm,
    weights_hbm,
    gate_hbm,
    conv_gate_hbm,
    conv_value_hbm,
    taps_hbm,
    wg_hbm,
    wu_hbm,
    wd_hbm,
    wo_hbm,
    half_hbm,
    gate_out,
    up_out,
    down_out,
    first_hbm,
    second_hbm,
    third_hbm,
    fourth_hbm,
    stream_in,
    grad_in,
    ids,
    weights,
    gate_in,
    conv_gate,
    conv_value,
    taps,
    half_out,
    first_out,
    second_out,
    third_out,
    fourth_out,
    toks_in,
    table,
    pick,
    scale,
    rel,
    rows,
    cot,
    wg,
    wu,
    wd,
    pre_g,
    pre_u,
    hidden,
    gg,
    ug,
    part_out,
    part_in,
    ret,
    back,
    col_out,
    col_in,
    total,
    gate_f,
    up_f,
    down_f,
    mix,
    mix_src,
    padded,
    conv_sum,
    halo_src,
    halo_dst,
    wo,
    far_half,
    strips,
    share_out,
    share_in,
    edge_src,
    edge_dst,
    in_sem,
    w_sem,
    out_sem,
    z_send,
    z_recv,
    t_send,
    t_recv,
    i_send,
    i_recv,
    f_send,
    f_recv,
    p_send,
    p_recv,
    r_send,
    r_recv,
    c_send,
    c_recv,
    m_send,
    m_recv,
    h_sem,
    g_send,
    g_recv,
    own_sem,
    d_send,
    d_recv,
    s_send,
    s_recv,
    b_send,
    b_recv,
    e_sem,
):
    me = lax.axis_index("sp")
    half = lax.axis_index("tp")
    other = 1 - half
    team = count // LAYERS
    place, layer = lax.rem(me, team), me // team
    side = layer // 2
    inner = lax.rem(layer + 1, LAYERS) >= 2
    outer = jnp.logical_not(inner)
    next_layer = layer + 1 - 2 * lax.rem(layer, 2)
    across_layer = 2 - side
    far_layer = 3 * (1 - side)
    toks, width = stream_in.shape
    slots = team * cap
    depth = taps.shape[0]
    top = ids.shape[0]

    def column(at):
        return (at * team + place, half)

    def teammate(i):
        return layer * team + lax.rem(place + i, team)

    firsts = []
    for n, (a, b) in enumerate(
        (
            (conv_gate_hbm, conv_gate),
            (conv_value_hbm, conv_value),
            (stream_hbm, stream_in),
            (ids_hbm, ids),
            (weights_hbm, weights),
            (grad_hbm, grad_in),
            (gate_hbm, gate_in),
            (taps_hbm, taps),
        )
    ):
        firsts.append(pltpu.make_async_copy(a, b, in_sem.at[n]))
        firsts[-1].start()
    loads = []
    for n, (a, b) in enumerate(((wg_hbm, wg), (wu_hbm, wu), (wd_hbm, wd))):
        load = pltpu.make_async_copy(a.at[0], b, w_sem.at[n])
        load.start()
        loads.append(load)
    if fused:
        load = pltpu.make_async_copy(wo_hbm, wo, w_sem.at[3])
        load.start()
        loads.append(load)

    after, before = lax.rem(me + 1, count), lax.rem(me + count - 1, count)
    barrier = pltpu.get_barrier_semaphore()

    def greet(device):
        pl.semaphore_signal(barrier, inc=1, device_id=device, device_id_type=MESH)

    greet(column(lax.rem(layer + 1, LAYERS)))
    greet(column(lax.rem(layer + 2, LAYERS)))
    greet(column(lax.rem(layer + 3, LAYERS)))

    @pl.loop(1, team)
    def _(i):
        greet((teammate(i), half))

    greet((me, other))
    greet((after, half))
    greet((before, half))
    for load in firsts:
        load.wait()
    pl.semaphore_wait(barrier, LAYERS - 1 + team - 1 + 3)

    def remote(src, dst, send, recv, device):
        return pltpu.make_async_remote_copy(
            src_ref=src,
            dst_ref=dst,
            send_sem=send,
            recv_sem=recv,
            device_id=device,
            device_id_type=MESH,
        )

    def block(k):
        return pl.ds(pl.multiple_of(k * cap, cap), cap)

    def piece(j, k):
        return pl.ds(pl.multiple_of(j * slots + k * cap, cap), cap)

    def group(j):
        return pl.ds(j * slots, slots)

    whole = (stream_in, grad_in)

    def blocks_of(which, j):
        return whole[which] if j == OWN else toks_in.at[which, j - 1]

    stretch = width // CHUNKS

    def hop(which, n, j, to, lands, c):
        at = pl.ds(c * stretch, stretch)
        return remote(
            blocks_of(which, j).at[:, at],
            toks_in.at[which, lands - 1, :, at],
            z_send.at[which, n],
            z_recv.at[which, lands - 1, c],
            column(to),
        )

    def own_to_next(which, c):
        return hop(which, 0, OWN, next_layer, NEXT, c)

    def own_to_across(which, c):
        return hop(which, 1, OWN, across_layer, ACROSS, c)

    def next_to_across(which, c):
        return hop(which, 2, NEXT, across_layer, FAR, c)

    def across_to_next(which, c):
        return hop(which, 3, ACROSS, next_layer, ACROSS, c)

    def far_to_next(which, c):
        return hop(which, 4, FAR, next_layer, FAR, c)

    def arrived(which, j):
        for c in range(CHUNKS):
            hop(which, 0, j, next_layer, j, c).wait_recv()

    def begin(copy, which):
        for c in range(CHUNKS):
            copy(which, c).start()

    def relay(*steps):
        for c in range(CHUNKS):
            for which, j, copy in steps:
                hop(which, 0, j, next_layer, j, c).wait_recv()
                copy(which, c).start()

    last = pl.ds(toks - 8, 8)
    halo_src[...] = conv_gate[last].astype(F32) * conv_value[last].astype(F32)
    halo = remote(halo_src, halo_dst, h_sem.at[0], h_sem.at[1], (after, half))
    halo.start()
    begin(own_to_next, 0)

    @pl.when(inner)
    def _():
        begin(own_to_across, 0)

    expert = lax.broadcasted_iota(jnp.int32, (count, toks), 0)
    hits = [ids[k : k + 1] == expert for k in range(top)]
    named = functools.reduce(jnp.logical_or, hits)
    named = jnp.where(named, 1.0, 0.0).astype(BF16)
    early = lax.broadcasted_iota(jnp.int32, (toks, toks), 0)
    late = lax.broadcasted_iota(jnp.int32, (toks, toks), 1)
    earlier = jnp.where(early < late, 1.0, 0.0).astype(BF16)
    spots = dot(named, earlier, 1, 0) + (expert * cap).astype(F32)
    table[OWN] = jnp.zeros(table.shape[1:], F32)
    for k in range(top):
        table[OWN, k : k + 1] = jnp.sum(jnp.where(hits[k], spots, 0.0), axis=0, keepdims=True)
        table[OWN, top + k : top + k + 1] = weights[k : k + 1]

    seen_as = jnp.where(inner, ACROSS, FAR)

    def table_copy(n, to, lands):
        return remote(
            table.at[OWN], table.at[lands], t_send.at[n], t_recv.at[lands], column(to)
        )

    tables = (
        table_copy(0, next_layer, NEXT),
        table_copy(1, across_layer, seen_as),
        table_copy(2, far_layer, seen_as),
    )
    for copy in tables:
        copy.start()

    begin(own_to_next, 1)

    base = (layer * slots).astype(F32)

    def choose(j):
        spot = lax.broadcasted_iota(jnp.int32, (slots, toks), 0).astype(F32)
        found = [table[j, k : k + 1] - base == spot for k in range(top)]
        pick[j] = jnp.where(functools.reduce(jnp.logical_or, found), 1.0, 0.0).astype(BF16)
        scale[j] = sum(
            jnp.sum(
                jnp.where(found[k], table[j, top + k : top + k + 1], 0.0), axis=1, keepdims=True
            )
            for k in range(top)
        )

    bufs = (rows, cot)

    def in_copy(which, j, i, at=slice(None)):
        return remote(
            rel.at[which, j, block(lax.rem(place + i, team)), at],
            bufs[which].at[half, piece(j, place), at],
            i_send.at[which, j],
            i_recv.at[which, j, i],
            (teammate(i), half),
        )

    def in_arrival(which, j, i):
        at = bufs[which].at[half, piece(j, lax.rem(place - i + team, team))]
        return remote(at, at, i_send.at[which, j], i_recv.at[which, j, i], (teammate(i), half))

    def pass_copy(which, j, i):
        at = bufs[which].at[half, piece(j, lax.rem(place - i + team, team))]
        return remote(at, at, f_send.at[which, j], f_recv.at[which, j], (me, other))

    def own_pass(which, j):
        return remote(
            rel.at[which, j, block(place)],
            bufs[which].at[half, piece(j, place)],
            f_send.at[which, j],
            f_recv.at[which, j],
            (me, other),
        )

    def passed(which, j):
        at = bufs[which].at[half, group(j)]
        return remote(at, at, f_send.at[which, j], f_recv.at[which, j], (me, other))

    def dealt(which, j):
        at = bufs[which].at[half, pl.ds(j * slots, slots - cap)]
        return remote(at, at, i_send.at[which, j], i_recv.at[which, j, 0], (me, other))

    def deal_chunk(which, j, c):
        at = pl.ds(c * stretch, stretch)
        chosen = dot(pick[j], blocks_of(which, j)[:, at], 1, 0)
        if which == 1:
            chosen = scale[j] * chosen
        rel[which, j, :, at] = chosen.astype(BF16)

        @pl.loop(1, team)
        def _(i):
            in_copy(which, j, i, at).start()

    def deal_own(which, j):
        own_pass(which, j).start()
        bufs[which][half, piece(j, place)] = rel[which, j, block(place)]

    def deal(which, j):
        for c in range(CHUNKS):
            deal_chunk(which, j, c)
        deal_own(which, j)

    def deal_arriving(which, j):
        for c in range(CHUNKS):
            hop(which, 0, j, next_layer, j, c).wait_recv()
            deal_chunk(which, j, c)
        deal_own(which, j)

    def gather(which, j):
        @pl.loop(1, team)
        def _(i):
            in_arrival(which, j, i).wait_recv()
            pass_copy(which, j, i).start()

        passed(which, j).wait_recv()

    mine_at = pl.ds(pl.multiple_of(half * width, width), width)
    other_at = pl.ds(pl.multiple_of(other * width, width), width)

    def part_copy(j):
        return remote(
            part_out.at[group(j)], part_in.at[group(j)], p_send.at[j], p_recv.at[j], (me, other)
        )

    def ret_copy(j, i):
        return remote(
            ret.at[piece(j, lax.rem(place + i, team))],
            back.at[piece(j, place)],
            r_send.at[j],
            r_recv.at[j],
            (teammate(i), half),
        )

    def ret_all(j):
        at = back.at[pl.ds(j * slots, slots - cap)]
        return remote(at, at, r_send.at[j], r_recv.at[j], (me, other))

    def ahead(j):
        gather(0, j)
        at = group(j)
        left, right = rows[0, at], rows[1, at]
        pre_g[at] = dot(left, wg[:width], 1, 0) + dot(right, wg[width:], 1, 0)
        pre_u[at] = dot(left, wu[:width], 1, 0) + dot(right, wu[width:], 1, 0)

    def behind(j):
        gather(1, j)
        at = group(j)
        grad = dot(cot[0, at], wd[:, :width], 1, 1) + dot(cot[1, at], wd[:, width:], 1, 1)
        pg, pu = pre_g[at], pre_u[at]
        sig = jax.nn.sigmoid(pg)
        silu = pg * sig
        hidden[at] = (silu * pu).astype(BF16)
        ug_now = (grad * silu).astype(BF16)
        gg_now = (grad * pu * sig * (1.0 + pg * (1.0 - sig))).astype(BF16)
        ug[at] = ug_now
        gg[at] = gg_now
        far = dot(gg_now, wg[other_at], 1, 1) + dot(ug_now, wu[other_at], 1, 1)
        part_out[at] = far.astype(BF16)
        part_copy(j).start()
        near = dot(gg_now, wg[mine_at], 1, 1) + dot(ug_now, wu[mine_at], 1, 1)
        near = near.astype(BF16).astype(F32)
        part_copy(j).wait_recv()
        ret[at] = (near + part_in[at].astype(F32)).astype(BF16)

    def send_back(j):
        @pl.loop(1, team)
        def _(i):
            ret_copy(j, i).start()

        back[piece(j, place)] = ret[piece(j, place)]

    def returned(j):
        ret_all(j).wait_recv()

    share = width // PARTS

    def cols(n):
        return pl.ds(n * share, share)

    def sum_copy(j, n):
        if j == NEXT:
            to, lands = next_layer, 0
        else:
            to = jnp.where(inner, across_layer, next_layer)
            lands = jnp.where(inner, j - 1, j + 1)
        return remote(
            col_out.at[j - 1, :, cols(n)],
            col_in.at[lands, :, cols(n)],
            c_send.at[j - 1],
            c_recv.at[lands, n],
            column(to),
        )

    def sum_arrival(lands, n):
        at = col_in.at[lands, :, cols(n)]
        return remote(at, at, c_send.at[0], c_recv.at[lands, n], column(next_layer))

    def partial(j, n):
        return dot(pick[j], back[group(j), cols(n)], 0, 0)

    def send_sums(j):
        for n in range(PARTS):
            col_out[j - 1, :, cols(n)] = partial(j, n).astype(BF16)
            sum_copy(j, n).start()

    def forward_sum(j, n):
        mine = partial(j, n)
        sum_arrival(j + 1, n).wait_recv()
        mine = mine + col_in[j + 1, :, cols(n)].astype(F32)
        col_out[j - 1, :, cols(n)] = mine.astype(BF16)
        sum_copy(j, n).start()

    choose(OWN)
    deal(0, OWN)
    deal(1, OWN)

    halo.wait_recv()
    prod = conv_gate[...].astype(F32) * conv_value[...].astype(F32)
    padded[8:] = prod
    padded[:8] = jnp.where(me == 0, 0.0, halo_dst[...])
    conv = jnp.zeros(prod.shape, F32)
    for tap in range(depth):
        start = 8 - (depth - 1) + tap
        conv = conv + taps[tap : tap + 1] * padded[start : start + toks]
    conv_sum[...] = conv
    mix_src[...] = (gate_in[...].astype(F32) * conv).astype(BF16)

    def mix_copy(j):
        return remote(
            mix_src,
            mix.at[pl.ds(pl.multiple_of(j * toks, toks), toks)],
            m_send.at[0],
            m_recv.at[0],
            (teammate(j), half),
        )

    def mix_all():
        at = mix.at[pl.ds(0, (team - 1) * toks)]
        return remote(at, at, m_send.at[0], m_recv.at[0], (me, other))

    def informed(j):
        table_copy(0, next_layer, j).wait_recv()
        choose(j)

    @pl.when(inner)
    def _():
        relay((0, NEXT, next_to_across), (0, ACROSS, across_to_next))

    @pl.when(outer)
    def _():
        arrived(0, NEXT)

    informed(NEXT)
    deal(0, NEXT)
    for load in loads:
        load.wait()

    @pl.when(inner)
    def _():
        relay((1, NEXT, next_to_across), (0, FAR, far_to_next))
        begin(own_to_across, 1)

    @pl.when(outer)
    def _():
        arrived(1, NEXT)

    deal(1, NEXT)
    ahead(OWN)
    behind(OWN)
    send_back(OWN)

    @pl.when(inner)
    def _():
        relay((1, FAR, far_to_next))

    ahead(NEXT)
    behind(NEXT)
    send_back(NEXT)

    @pl.when(outer)
    def _():
        arrived(0, ACROSS)

    informed(ACROSS)
    deal(0, ACROSS)
    returned(OWN)
    total[...] = dot(pick[OWN], back[group(OWN)], 0, 0)
    returned(NEXT)

    @pl.when(outer)
    def _():
        send_sums(NEXT)
        arrived(0, FAR)

    informed(FAR)
    deal(0, FAR)

    @pl.when(inner)
    def _():
        relay((1, ACROSS, across_to_next))

    ahead(ACROSS)

    @pl.when(outer)
    def _():
        deal_arriving(1, FAR)

    @pl.when(inner)
    def _():
        deal(1, FAR)

    ahead(FAR)

    @pl.when(outer)
    def _():
        deal_arriving(1, ACROSS)

    @pl.when(inner)
    def _():
        deal(1, ACROSS)

    behind(FAR)
    send_back(FAR)
    behind(ACROSS)
    send_back(ACROSS)

    if fused:

        @pl.loop(1, team)
        def _(j):
            mix_copy(j).start()

        mix[pl.ds(0, toks)] = mix_src[...]

    returned(FAR)

    @pl.when(outer)
    def _():
        send_sums(FAR)

    hid_part = hidden.shape[1] // PARTS
    deep_part = width // PARTS

    def weights_part(n):
        to = pl.ds(n * hid_part, hid_part)
        x = hidden[:, to].T
        for h in range(2):
            down_f[to, h * width : (h + 1) * width] = dot(x, cot[h], 1, 0).astype(BF16)

        @pl.loop(0, 2)
        def _(h):
            to = pl.ds(pl.multiple_of(h * width + n * deep_part, deep_part), deep_part)
            x = rows[h, :, n * deep_part : (n + 1) * deep_part].T
            gate_f[to] = dot(x, gg[...], 1, 0).astype(BF16)
            up_f[to] = dot(x, ug[...], 1, 0).astype(BF16)

    for n in range(PARTS):

        @pl.when(inner)
        def _():
            forward_sum(FAR, n)
            if n >= 2:
                forward_sum(NEXT, n - 2)

        weights_part(n)

    stores = [
        pltpu.make_async_copy(gate_f, gate_out.at[0], out_sem.at[0]),
        pltpu.make_async_copy(up_f, up_out.at[0], out_sem.at[1]),
        pltpu.make_async_copy(down_f, down_out.at[0], out_sem.at[2]),
    ]
    for store in stores:
        store.start()

    per = LAYERS // 2
    blk = width // (team * per)

    def band(b):
        return pl.ds(b * blk, blk)

    def spot(h, m, size):
        return pl.ds(pl.multiple_of((h * per + m) * blk, blk), size)

    def stripe(j):
        return pl.ds(pl.multiple_of(j * toks, toks), toks)

    def piece_copy(b, j, m):
        return remote(
            half_out.at[:, band(b)],
            strips.at[stripe(j), spot(half, m, blk)],
            g_send.at[m],
            g_recv.at[m],
            (teammate(j), half),
        )

    def own_piece(b, m):
        return remote(
            half_out.at[:, band(b)],
            strips.at[stripe(0), spot(half, m, blk)],
            own_sem.at[0, m],
            own_sem.at[1, m],
            (me, other),
        )

    def whole_copy(n):
        return remote(
            half_out.at[:, cols(n)], far_half.at[:, cols(n)], b_send.at[0], b_recv.at[0], (me, other)
        )

    def whole_all():
        return remote(half_out, far_half, b_send.at[0], b_recv.at[0], (me, other))

    def handed(j, m):
        at = strips.at[stripe(j), spot(half, m, blk)]
        return remote(at, at, d_send.at[m], d_recv.at[m], (me, other))

    def layer_copy(at):
        return remote(
            share_out.at[at], share_in.at[layer], s_send.at[at], s_recv.at[layer], column(at)
        )

    def layer_arrival(at):
        return remote(
            share_in.at[at], share_in.at[at], s_send.at[at], s_recv.at[at], column(at)
        )

    def hand_over(m):
        pieces_all(m).wait_recv()

        @pl.loop(1, team)
        def _(j):
            handed(j, m).start()

    def pieces_all(m):
        at = strips.at[pl.ds(toks, (team - 1) * toks), band(m)]
        return remote(at, at, g_send.at[m], g_recv.at[m], (me, other))

    def handed_all(m):
        at = strips.at[pl.ds(toks, (team - 1) * toks), band(m)]
        return remote(at, at, d_send.at[m], d_recv.at[m], (me, other))

    def settle(n):
        sum_arrival(0, n).wait_recv()
        now = total[:, cols(n)] + col_in[0, :, cols(n)].astype(F32)
        half_out[:, cols(n)] = (grad_in[:, cols(n)].astype(F32) + now).astype(BF16)
        if fused:
            whole_copy(n).start()
            for b in range(n * share // blk, (n + 1) * share // blk):
                j, m = lax.rem(b % team - place + team, team), b // team

                @pl.when(j > 0)
                def _():
                    piece_copy(b, j, m).start()

                @pl.when(j == 0)
                def _():
                    own_piece(b, m).start()
                    strips[stripe(0), spot(half, m, blk)] = half_out[:, band(b)]

    def settle_inner(n):
        sum_arrival(1, n).wait_recv()
        total[:, cols(n)] += col_in[1, :, cols(n)].astype(F32)
        settle(n)

    returned(ACROSS)

    @pl.when(outer)
    def _():
        send_sums(ACROSS)

    @pl.when(inner)
    def _():
        for n in range(PARTS):
            forward_sum(ACROSS, n)
            if n < 2:
                forward_sum(NEXT, PARTS - 2 + n)
            if n >= 2:
                settle_inner(n - 2)
        settle_inner(PARTS - 2)
        if fused:
            hand_over(0)
        settle_inner(PARTS - 1)

    @pl.when(outer)
    def _():
        for n in range(PARTS - 1):
            settle(n)
        if fused:
            hand_over(0)
        settle(PARTS - 1)

    def edge_copy():
        return remote(edge_src, edge_dst, e_sem.at[0], e_sem.at[1], (before, half))

    def mixer_grad():
        mixed = dot(half_out[...], wo[mine_at], 1, 0)
        whole_all().wait_recv()
        mixed = (mixed + dot(far_half[...], wo[other_at], 1, 0)).astype(BF16)
        wide = mixed.astype(F32)
        inner_conv = wide * gate_in[...].astype(F32)
        edge_src[...] = inner_conv[:8]
        edge_copy().start()
        padded[:toks] = inner_conv
        second_out[...] = (wide * conv_sum[...]).astype(BF16)

    def conv_grads():
        edge_copy().wait_recv()
        padded[toks:] = jnp.where(me == count - 1, 0.0, edge_dst[...])
        prod_grad = jnp.zeros((toks, taps.shape[1]), F32)
        for tap in range(depth):
            start = depth - 1 - tap
            prod_grad = prod_grad + taps[tap : tap + 1] * padded[start : start + toks]
        third_out[...] = (prod_grad * conv_value[...].astype(F32)).astype(BF16)
        fourth_out[...] = (prod_grad * conv_gate[...].astype(F32)).astype(BF16)

    def strips_in(m):
        own_piece(0, m).wait_recv()
        handed_all(m).wait_recv()

    def shares_out(m):
        for at in range(m, LAYERS, per):
            now = dot(strips[:, band(at)].T, mix[...], 1, 0)

            @pl.when(layer == at)
            def _():
                first_out[...] = now

            @pl.when(layer != at)
            def _():
                share_out[at] = now.astype(BF16)
                layer_copy(at).start()

    def shares_in():
        for i in (1, 3, 2):
            at = lax.rem(layer + i, LAYERS)
            layer_arrival(at).wait_recv()
            first_out[...] += share_in[at].astype(F32)

    def hopped(which, n):
        at = toks_in.at[which, 0]
        return remote(at, at, z_send.at[which, n], z_recv.at[which, 0, 0], column(next_layer))

    def summed(j):
        at = col_out.at[j - 1]
        return remote(at, at, c_send.at[j - 1], c_recv.at[0, 0], column(next_layer))

    def drain():
        for which in range(2):
            hopped(which, 0).wait_send()
            for j in range(LAYERS):
                passed(which, j).wait_send()
                dealt(which, j).wait_send()

        @pl.when(inner)
        def _():
            for which in range(2):
                for n in range(1, 5):
                    hopped(which, n).wait_send()

        for j in range(LAYERS):
            part_copy(j).wait_send()
            ret_all(j).wait_send()
        for j in (NEXT, ACROSS, FAR):
            summed(j).wait_send()
        for copy in tables:
            copy.wait_send()
        halo.wait_send()
        if fused:
            edge_copy().wait_send()
            whole_all().wait_send()
            mix_all().wait_send()
            for m in range(per):
                own_piece(0, m).wait_send()
                handed_all(m).wait_send()
                pieces_all(m).wait_send()

    def keep(n, src, dst):
        stores.append(pltpu.make_async_copy(src, dst, out_sem.at[n]))
        stores[-1].start()

    keep(3, half_out, half_hbm)
    if fused:

        mix_all().wait_recv()
        for m in range(per):
            strips_in(m)
            shares_out(m)
            if m == 0:
                mixer_grad()
            if m + 1 < per:
                hand_over(m + 1)
        conv_grads()
        keep(5, second_out, second_hbm)
        keep(6, third_out, third_hbm)
        keep(7, fourth_out, fourth_hbm)
        drain()
        shares_in()
        keep(4, first_out, first_hbm)
        for i in range(1, LAYERS):
            layer_copy(lax.rem(layer + i, LAYERS)).wait_send()
    else:
        drain()
        keep(4, conv_sum, first_hbm)
        keep(5, mix_src, second_hbm)
        keep(6, halo_src, third_hbm)
        keep(7, halo_dst, fourth_hbm)

    def finish():
        for store in stores:
            store.wait()

    finish()


def expert_pass(
    fused,
    stream,
    out_grad,
    ids,
    weights,
    gate_in,
    conv_gate,
    conv_value,
    taps,
    w_gate,
    w_up,
    w_down,
    w_out,
):
    toks, width = stream.shape
    chans = gate_in.shape[1]
    count = lax.axis_size("sp")
    cap = 4 * toks // count
    team = count // LAYERS
    slots = team * cap
    tall = LAYERS * slots
    deep, hid = w_gate.shape[1:]
    blk = deep // count
    if fused:
        extra = (((blk, chans), F32),) + (((toks, chans), BF16),) * 3
    else:
        extra = (((toks, chans), F32), ((toks, chans), BF16)) + (((8, chans), F32),) * 2
    crew = team if fused else 1
    anywhere = pl.BlockSpec(memory_space=pl.ANY)
    dma = pltpu.SemaphoreType.DMA
    return pl.pallas_call(
        functools.partial(expert_kernel, count, cap, fused),
        out_shape=(
            jax.ShapeDtypeStruct((toks, width), BF16),
            jax.ShapeDtypeStruct((1, deep, hid), BF16),
            jax.ShapeDtypeStruct((1, deep, hid), BF16),
            jax.ShapeDtypeStruct((1, hid, deep), BF16),
        )
        + tuple(jax.ShapeDtypeStruct(*one) for one in extra),
        in_specs=[anywhere] * 12,
        out_specs=(anywhere,) * 8,
        scratch_shapes=[
            pltpu.VMEM((toks, width), BF16),
            pltpu.VMEM((toks, width), BF16),
            pltpu.VMEM(ids.shape, ids.dtype),
            pltpu.VMEM(weights.shape, F32),
            pltpu.VMEM((toks, chans), BF16),
            pltpu.VMEM((toks, chans), BF16),
            pltpu.VMEM((toks, chans), BF16),
            pltpu.VMEM(taps.shape, F32),
            pltpu.VMEM((toks, width), BF16),
            pltpu.VMEM((blk, chans), F32),
            pltpu.VMEM((toks, chans), BF16),
            pltpu.VMEM((toks, chans), BF16),
            pltpu.VMEM((toks, chans), BF16),
            pltpu.VMEM((2, LAYERS - 1, toks, width), BF16),
            pltpu.VMEM((LAYERS, 8, toks), F32),
            pltpu.VMEM((LAYERS, slots, toks), BF16),
            pltpu.VMEM((LAYERS, slots, 1), F32),
            pltpu.VMEM((2, LAYERS, slots, width), BF16),
            pltpu.VMEM((2, tall, width), BF16),
            pltpu.VMEM((2, tall, width), BF16),
            pltpu.VMEM((deep, hid), BF16),
            pltpu.VMEM((deep, hid), BF16),
            pltpu.VMEM((hid, deep), BF16),
            pltpu.VMEM((tall, hid), F32),
            pltpu.VMEM((tall, hid), F32),
            pltpu.VMEM((tall, hid), BF16),
            pltpu.VMEM((tall, hid), BF16),
            pltpu.VMEM((tall, hid), BF16),
            pltpu.VMEM((tall, width), BF16),
            pltpu.VMEM((tall, width), BF16),
            pltpu.VMEM((tall, width), BF16),
            pltpu.VMEM((tall, width), BF16),
            pltpu.VMEM((LAYERS - 1, toks, width), BF16),
            pltpu.VMEM((5, toks, width), BF16),
            pltpu.VMEM((toks, width), F32),
            pltpu.VMEM((deep, hid), BF16),
            pltpu.VMEM((deep, hid), BF16),
            pltpu.VMEM((hid, deep), BF16),
            pltpu.VMEM((crew * toks, chans), BF16),
            pltpu.VMEM((toks, chans), BF16),
            pltpu.VMEM((toks + 8, chans), F32),
            pltpu.VMEM((toks, chans), F32),
            pltpu.VMEM((8, chans), F32),
            pltpu.VMEM((8, chans), F32),
            pltpu.VMEM((deep, chans) if fused else (16, 128), BF16),
            pltpu.VMEM((toks, width) if fused else (16, 128), BF16),
            pltpu.VMEM((team * toks, LAYERS * blk) if fused else (16, 128), BF16),
            pltpu.VMEM((LAYERS, blk, chans), BF16),
            pltpu.VMEM((LAYERS, blk, chans), BF16),
            pltpu.VMEM((8, chans), F32),
            pltpu.VMEM((8, chans), F32),
            dma((8,)),
            dma((4,)),
            dma((8,)),
            dma((2, 5)),
            dma((2, LAYERS - 1, CHUNKS)),
            dma((3,)),
            dma((LAYERS,)),
            dma((2, LAYERS)),
            dma((2, LAYERS, team)),
            dma((2, LAYERS)),
            dma((2, LAYERS)),
            dma((LAYERS,)),
            dma((LAYERS,)),
            dma((LAYERS,)),
            dma((LAYERS,)),
            dma((LAYERS - 1,)),
            dma((5, PARTS)),
            dma((1,)),
            dma((1,)),
            dma((2,)),
            dma((LAYERS // 2,)),
            dma((LAYERS // 2,)),
            dma((2, LAYERS // 2)),
            dma((LAYERS // 2,)),
            dma((LAYERS // 2,)),
            dma((LAYERS,)),
            dma((LAYERS,)),
            dma((1,)),
            dma((1,)),
            dma((2,)),
        ],
        compiler_params=pltpu.CompilerParams(
            collective_id=0, has_side_effects=True, vmem_limit_bytes=62 * 1024 * 1024
        ),
    )(
        stream,
        out_grad,
        ids,
        weights,
        gate_in,
        conv_gate,
        conv_value,
        taps,
        w_gate,
        w_up,
        w_down,
        w_out,
    )


def publish_kernel(small, large, *refs):
    total = small + large
    ins, outs, refs = refs[:total], refs[total : 2 * total], refs[2 * total :]
    held, wide, (in_sem, out_sem) = refs[:total], refs[total : total + large], refs[total + large :]

    def spots(k):
        if k < small:
            return [(0, slice(None), slice(None))]
        size = held[k].shape[0] // PARTS
        return [(n, (0, pl.ds(n * size, size)), pl.ds(n * size, size)) for n in range(PARTS)]

    def load(k, n, outer_at, at):
        src = ins[k] if k < small else ins[k].at[outer_at]
        dst = held[k] if k < small else held[k].at[at]
        return pltpu.make_async_copy(src, dst, in_sem.at[k, n])

    def store(k, n, outer_at, at):
        src = held[k] if k < small else wide[k - small].at[at]
        dst = outs[k] if k < small else outs[k].at[outer_at]
        return pltpu.make_async_copy(src, dst, out_sem.at[k, n])

    order = list(range(small, total)) + list(range(small))
    steps = [(k, *spot) for k in order for spot in spots(k)]
    for step in steps:
        load(*step).start()
    for step in steps:
        load(*step).wait()
        k, at = step[0], step[3]
        if k >= small:
            wide[k - small][at] = held[k][at].astype(F32)
        store(*step).start()
    for step in steps:
        store(*step).wait()


def publish(smalls, larges):
    anywhere = pl.BlockSpec(memory_space=pl.ANY)
    dma = pltpu.SemaphoreType.DMA
    total = len(smalls) + len(larges)
    outs = [jax.ShapeDtypeStruct(x.shape, x.dtype) for x in smalls]
    outs += [jax.ShapeDtypeStruct(x.shape, F32) for x in larges]
    return pl.pallas_call(
        functools.partial(publish_kernel, len(smalls), len(larges)),
        out_shape=tuple(outs),
        in_specs=[anywhere] * total,
        out_specs=(anywhere,) * total,
        scratch_shapes=[pltpu.VMEM(x.shape, x.dtype) for x in smalls]
        + [pltpu.VMEM(x.shape[1:], BF16) for x in larges]
        + [pltpu.VMEM(x.shape[1:], F32) for x in larges]
        + [dma((total, PARTS)), dma((total, PARTS))],
        compiler_params=pltpu.CompilerParams(vmem_limit_bytes=62 * 1024 * 1024),
    )(*smalls, *larges)


def shards(
    stream,
    out_grad,
    gate_in,
    conv_gate,
    conv_value,
    taps,
    w_out,
    route_ids,
    route_weights,
    w_gate,
    w_up,
    w_down,
):
    tok_rows, channels = conv_gate.shape
    me = lax.axis_index("sp")
    depth = taps.shape[0]
    fused = w_out.shape[0] // lax.axis_size("sp") % 128 == 0
    stream_half, gate_w_grad, up_w_grad, down_w_grad, *extra = expert_pass(
        fused,
        stream,
        out_grad,
        route_ids.T,
        route_weights.T,
        gate_in,
        conv_gate,
        conv_value,
        taps,
        w_gate,
        w_up,
        w_down,
        w_out,
    )
    if fused:
        out_proj_grad, *chan_grads = extra
        smalls = (stream_half, *chan_grads, out_proj_grad)
        return publish(smalls, (gate_w_grad, up_w_grad, down_w_grad))
    conv_sum, mixer_out = extra[:2]
    stream_whole = lax.all_gather(stream_half, "tp", axis=1, tiled=True)
    mixer_grad = dot(stream_whole, w_out, 1, 0).astype(BF16)
    out_proj_grad = lax.psum_scatter(
        dot(stream_whole, mixer_out, 0, 0).astype(BF16), "sp", scatter_dimension=0, tiled=True
    ).astype(F32)
    first = mixer_grad[: depth - 1].astype(F32) * gate_in[: depth - 1].astype(F32)
    halo = passed_along(first, "sp", -1)
    mixer_wide = mixer_grad.astype(jnp.float32)
    gate_in_grad = (mixer_wide * conv_sum).astype(jnp.bfloat16)
    conv_inner = mixer_wide * gate_in.astype(jnp.float32)
    right_rows = jnp.where(me == lax.axis_size("sp") - 1, 0.0, halo[: depth - 1])
    padded_back = jnp.concatenate([conv_inner, right_rows], axis=0)
    prod_grad = jnp.zeros((tok_rows, channels), jnp.float32)
    for tap_index in range(depth):
        offset = depth - 1 - tap_index
        prod_grad = prod_grad + taps[tap_index][None, :] * padded_back[offset : offset + tok_rows]
    conv_gate_grad = (prod_grad * conv_value.astype(jnp.float32)).astype(jnp.bfloat16)
    conv_value_grad = (prod_grad * conv_gate.astype(jnp.float32)).astype(jnp.bfloat16)
    return (
        stream_half,
        gate_in_grad,
        conv_gate_grad,
        conv_value_grad,
        out_proj_grad,
        gate_w_grad.astype(F32),
        up_w_grad.astype(F32),
        down_w_grad.astype(F32),
    )


def solution(mesh):
    placed = (
        P("sp", "tp"),
        P("sp", "tp"),
        P("sp", "tp"),
        P("sp", "tp"),
        P("sp", "tp"),
        P(None, "tp"),
        P(None, "tp"),
        P("sp", None),
        P("sp", None),
        P("sp", None, "tp"),
        P("sp", None, "tp"),
        P("sp", "tp", None),
    )
    return jax.shard_map(
        shards,
        mesh=mesh,
        in_specs=placed,
        out_specs=(
            P("sp", "tp"),
            P("sp", "tp"),
            P("sp", "tp"),
            P("sp", "tp"),
            P("sp", "tp"),
            P("sp", None, "tp"),
            P("sp", None, "tp"),
            P("sp", "tp", None),
        ),
        check_vma=False,
    )
```

```python
import functools

import jax
import jax.numpy as jnp
from jax import lax
from jax.experimental import pallas as pl
from jax.experimental.pallas import tpu as pltpu
from jax.sharding import PartitionSpec as P

MESH = pl.DeviceIdType.MESH
LAYERS = 4
PARTS = 4
CHUNKS = 4
F32 = jnp.float32
BF16 = jnp.bfloat16
OWN, NEXT, ACROSS, FAR = 0, 1, 2, 3


def passed_along(shard, axis, by):
    count = lax.axis_size(axis)
    pairs = [(i, i + by) for i in range(count) if 0 <= i + by < count]
    return lax.ppermute(shard, axis, pairs)


def dot(a, b, ca, cb):
    return lax.dot_general(a, b, (((ca,), (cb,)), ((), ())), preferred_element_type=F32)


def expert_kernel(
    count,
    cap,
    fused,
    stream_hbm,
    grad_hbm,
    ids_hbm,
    weights_hbm,
    gate_hbm,
    conv_gate_hbm,
    conv_value_hbm,
    taps_hbm,
    wg_hbm,
    wu_hbm,
    wd_hbm,
    wo_hbm,
    half_hbm,
    gate_out,
    up_out,
    down_out,
    first_hbm,
    second_hbm,
    third_hbm,
    fourth_hbm,
    stream_in,
    grad_in,
    ids,
    weights,
    gate_in,
    conv_gate,
    conv_value,
    taps,
    half_out,
    first_out,
    second_out,
    third_out,
    fourth_out,
    toks_in,
    table,
    pick,
    scale,
    rel,
    rows,
    cot,
    wg,
    wu,
    wd,
    pre_g,
    pre_u,
    hidden,
    gg,
    ug,
    part_out,
    part_in,
    ret,
    back,
    col_out,
    col_in,
    total,
    gate_f,
    up_f,
    down_f,
    mix,
    mix_src,
    padded,
    conv_sum,
    halo_src,
    halo_dst,
    wo,
    far_half,
    strips,
    share_out,
    share_in,
    edge_src,
    edge_dst,
    in_sem,
    w_sem,
    out_sem,
    z_send,
    z_recv,
    t_send,
    t_recv,
    i_send,
    i_recv,
    f_send,
    f_recv,
    p_send,
    p_recv,
    r_send,
    r_recv,
    c_send,
    c_recv,
    m_send,
    m_recv,
    h_sem,
    g_send,
    g_recv,
    own_sem,
    d_send,
    d_recv,
    s_send,
    s_recv,
    b_send,
    b_recv,
    e_sem,
):
    me = lax.axis_index("sp")
    half = lax.axis_index("tp")
    other = 1 - half
    team = count // LAYERS
    place, layer = lax.rem(me, team), me // team
    side = layer // 2
    inner = lax.rem(layer + 1, LAYERS) >= 2
    outer = jnp.logical_not(inner)
    next_layer = layer + 1 - 2 * lax.rem(layer, 2)
    across_layer = 2 - side
    far_layer = 3 * (1 - side)
    toks, width = stream_in.shape
    slots = team * cap
    depth = taps.shape[0]
    top = ids.shape[0]

    def column(at):
        return (at * team + place, half)

    def teammate(i):
        return layer * team + lax.rem(place + i, team)

    firsts = []
    for n, (a, b) in enumerate(
        (
            (conv_gate_hbm, conv_gate),
            (conv_value_hbm, conv_value),
            (stream_hbm, stream_in),
            (ids_hbm, ids),
            (weights_hbm, weights),
            (grad_hbm, grad_in),
            (gate_hbm, gate_in),
            (taps_hbm, taps),
        )
    ):
        firsts.append(pltpu.make_async_copy(a, b, in_sem.at[n]))
        firsts[-1].start()
    loads = []
    for n, (a, b) in enumerate(((wg_hbm, wg), (wu_hbm, wu), (wd_hbm, wd))):
        load = pltpu.make_async_copy(a.at[0], b, w_sem.at[n])
        load.start()
        loads.append(load)
    if fused:
        load = pltpu.make_async_copy(wo_hbm, wo, w_sem.at[3])
        load.start()
        loads.append(load)

    after, before = lax.rem(me + 1, count), lax.rem(me + count - 1, count)
    barrier = pltpu.get_barrier_semaphore()

    def greet(device):
        pl.semaphore_signal(barrier, inc=1, device_id=device, device_id_type=MESH)

    greet(column(lax.rem(layer + 1, LAYERS)))
    greet(column(lax.rem(layer + 2, LAYERS)))
    greet(column(lax.rem(layer + 3, LAYERS)))

    @pl.loop(1, team)
    def _(i):
        greet((teammate(i), half))

    greet((me, other))
    greet((after, half))
    greet((before, half))
    for load in firsts:
        load.wait()
    pl.semaphore_wait(barrier, LAYERS - 1 + team - 1 + 3)

    def remote(src, dst, send, recv, device):
        return pltpu.make_async_remote_copy(
            src_ref=src,
            dst_ref=dst,
            send_sem=send,
            recv_sem=recv,
            device_id=device,
            device_id_type=MESH,
        )

    def block(k):
        return pl.ds(pl.multiple_of(k * cap, cap), cap)

    def piece(j, k):
        return pl.ds(pl.multiple_of(j * slots + k * cap, cap), cap)

    def group(j):
        return pl.ds(j * slots, slots)

    whole = (stream_in, grad_in)

    def blocks_of(which, j):
        return whole[which] if j == OWN else toks_in.at[which, j - 1]

    stretch = width // CHUNKS

    def hop(which, n, j, to, lands, c):
        at = pl.ds(c * stretch, stretch)
        return remote(
            blocks_of(which, j).at[:, at],
            toks_in.at[which, lands - 1, :, at],
            z_send.at[which, n],
            z_recv.at[which, lands - 1, c],
            column(to),
        )

    def own_to_next(which, c):
        return hop(which, 0, OWN, next_layer, NEXT, c)

    def own_to_across(which, c):
        return hop(which, 1, OWN, across_layer, ACROSS, c)

    def next_to_across(which, c):
        return hop(which, 2, NEXT, across_layer, FAR, c)

    def across_to_next(which, c):
        return hop(which, 3, ACROSS, next_layer, ACROSS, c)

    def far_to_next(which, c):
        return hop(which, 4, FAR, next_layer, FAR, c)

    def arrived(which, j):
        for c in range(CHUNKS):
            hop(which, 0, j, next_layer, j, c).wait_recv()

    def begin(copy, which):
        for c in range(CHUNKS):
            copy(which, c).start()

    def relay(*steps):
        for c in range(CHUNKS):
            for which, j, copy in steps:
                hop(which, 0, j, next_layer, j, c).wait_recv()
                copy(which, c).start()

    last = pl.ds(toks - 8, 8)
    halo_src[...] = conv_gate[last].astype(F32) * conv_value[last].astype(F32)
    halo = remote(halo_src, halo_dst, h_sem.at[0], h_sem.at[1], (after, half))
    halo.start()
    begin(own_to_next, 0)

    @pl.when(inner)
    def _():
        begin(own_to_across, 0)

    expert = lax.broadcasted_iota(jnp.int32, (count, toks), 0)
    hits = [ids[k : k + 1] == expert for k in range(top)]
    named = functools.reduce(jnp.logical_or, hits)
    named = jnp.where(named, 1.0, 0.0).astype(BF16)
    early = lax.broadcasted_iota(jnp.int32, (toks, toks), 0)
    late = lax.broadcasted_iota(jnp.int32, (toks, toks), 1)
    earlier = jnp.where(early < late, 1.0, 0.0).astype(BF16)
    spots = dot(named, earlier, 1, 0) + (expert * cap).astype(F32)
    table[OWN] = jnp.zeros(table.shape[1:], F32)
    for k in range(top):
        table[OWN, k : k + 1] = jnp.sum(jnp.where(hits[k], spots, 0.0), axis=0, keepdims=True)
        table[OWN, top + k : top + k + 1] = weights[k : k + 1]

    seen_as = jnp.where(inner, ACROSS, FAR)

    def table_copy(n, to, lands):
        return remote(
            table.at[OWN], table.at[lands], t_send.at[n], t_recv.at[lands], column(to)
        )

    tables = (
        table_copy(0, next_layer, NEXT),
        table_copy(1, across_layer, seen_as),
        table_copy(2, far_layer, seen_as),
    )
    for copy in tables:
        copy.start()

    begin(own_to_next, 1)

    base = (layer * slots).astype(F32)

    def choose(j):
        spot = lax.broadcasted_iota(jnp.int32, (slots, toks), 0).astype(F32)
        found = [table[j, k : k + 1] - base == spot for k in range(top)]
        pick[j] = jnp.where(functools.reduce(jnp.logical_or, found), 1.0, 0.0).astype(BF16)
        scale[j] = sum(
            jnp.sum(
                jnp.where(found[k], table[j, top + k : top + k + 1], 0.0), axis=1, keepdims=True
            )
            for k in range(top)
        )

    bufs = (rows, cot)

    def in_copy(which, j, i, at=slice(None)):
        return remote(
            rel.at[which, j, block(lax.rem(place + i, team)), at],
            bufs[which].at[half, piece(j, place), at],
            i_send.at[which, j],
            i_recv.at[which, j, i],
            (teammate(i), half),
        )

    def in_arrival(which, j, i):
        at = bufs[which].at[half, piece(j, lax.rem(place - i + team, team))]
        return remote(at, at, i_send.at[which, j], i_recv.at[which, j, i], (teammate(i), half))

    def pass_copy(which, j, i):
        at = bufs[which].at[half, piece(j, lax.rem(place - i + team, team))]
        return remote(at, at, f_send.at[which, j], f_recv.at[which, j], (me, other))

    def own_pass(which, j):
        return remote(
            rel.at[which, j, block(place)],
            bufs[which].at[half, piece(j, place)],
            f_send.at[which, j],
            f_recv.at[which, j],
            (me, other),
        )

    def passed(which, j):
        at = bufs[which].at[half, group(j)]
        return remote(at, at, f_send.at[which, j], f_recv.at[which, j], (me, other))

    def dealt(which, j):
        at = bufs[which].at[half, pl.ds(j * slots, slots - cap)]
        return remote(at, at, i_send.at[which, j], i_recv.at[which, j, 0], (me, other))

    def deal_chunk(which, j, c):
        at = pl.ds(c * stretch, stretch)
        chosen = dot(pick[j], blocks_of(which, j)[:, at], 1, 0)
        if which == 1:
            chosen = scale[j] * chosen
        rel[which, j, :, at] = chosen.astype(BF16)

        @pl.loop(1, team)
        def _(i):
            in_copy(which, j, i, at).start()

    def deal_own(which, j):
        own_pass(which, j).start()
        bufs[which][half, piece(j, place)] = rel[which, j, block(place)]

    def deal(which, j):
        for c in range(CHUNKS):
            deal_chunk(which, j, c)
        deal_own(which, j)

    def deal_arriving(which, j):
        for c in range(CHUNKS):
            hop(which, 0, j, next_layer, j, c).wait_recv()
            deal_chunk(which, j, c)
        deal_own(which, j)

    def gather(which, j):
        @pl.loop(1, team)
        def _(i):
            in_arrival(which, j, i).wait_recv()
            pass_copy(which, j, i).start()

        passed(which, j).wait_recv()

    mine_at = pl.ds(pl.multiple_of(half * width, width), width)
    other_at = pl.ds(pl.multiple_of(other * width, width), width)

    def part_copy(j):
        return remote(
            part_out.at[group(j)], part_in.at[group(j)], p_send.at[j], p_recv.at[j], (me, other)
        )

    def side_of(h):
        return pl.ds(h * (width // 2), width // 2)

    def ret_copy(j, i, h):
        return remote(
            ret.at[piece(j, lax.rem(place + i, team)), side_of(h)],
            back.at[piece(j, place), side_of(h)],
            r_send.at[j, h],
            r_recv.at[j, h],
            (teammate(i), half),
        )

    def ret_all(j, h):
        at = back.at[pl.ds(j * slots, slots - cap), side_of(h)]
        return remote(at, at, r_send.at[j, h], r_recv.at[j, h], (me, other))

    def ahead(j):
        gather(0, j)
        at = group(j)
        left, right = rows[0, at], rows[1, at]
        pre_g[at] = dot(left, wg[:width], 1, 0) + dot(right, wg[width:], 1, 0)
        pre_u[at] = dot(left, wu[:width], 1, 0) + dot(right, wu[width:], 1, 0)

    def behind(j):
        gather(1, j)
        at = group(j)
        grad = dot(cot[0, at], wd[:, :width], 1, 1) + dot(cot[1, at], wd[:, width:], 1, 1)
        pg, pu = pre_g[at], pre_u[at]
        sig = jax.nn.sigmoid(pg)
        silu = pg * sig
        hidden[at] = (silu * pu).astype(BF16)
        ug_now = (grad * silu).astype(BF16)
        gg_now = (grad * pu * sig * (1.0 + pg * (1.0 - sig))).astype(BF16)
        ug[at] = ug_now
        gg[at] = gg_now
        far = dot(gg_now, wg[other_at], 1, 1) + dot(ug_now, wu[other_at], 1, 1)
        part_out[at] = far.astype(BF16)
        part_copy(j).start()
        near = dot(gg_now, wg[mine_at], 1, 1) + dot(ug_now, wu[mine_at], 1, 1)
        near = near.astype(BF16).astype(F32)
        part_copy(j).wait_recv()
        ret[at] = (near + part_in[at].astype(F32)).astype(BF16)

    def send_back(j):
        for h in range(2):

            @pl.loop(1, team)
            def _(i):
                ret_copy(j, i, h).start()

        back[piece(j, place)] = ret[piece(j, place)]

    def returned(j):
        for h in range(2):
            ret_all(j, h).wait_recv()

    share = width // PARTS

    def cols(n):
        return pl.ds(n * share, share)

    def sum_copy(j, n):
        if j == NEXT:
            to, lands = next_layer, 0
        else:
            to = jnp.where(inner, across_layer, next_layer)
            lands = jnp.where(inner, j - 1, j + 1)
        return remote(
            col_out.at[j - 1, :, cols(n)],
            col_in.at[lands, :, cols(n)],
            c_send.at[j - 1],
            c_recv.at[lands, n],
            column(to),
        )

    def sum_arrival(lands, n):
        at = col_in.at[lands, :, cols(n)]
        return remote(at, at, c_send.at[0], c_recv.at[lands, n], column(next_layer))

    def partial(j, n):
        return dot(pick[j], back[group(j), cols(n)], 0, 0)

    def send_sums(j, fresh=False):
        for n in range(PARTS):
            if fresh and n % (PARTS // 2) == 0:
                ret_all(j, n // (PARTS // 2)).wait_recv()
            col_out[j - 1, :, cols(n)] = partial(j, n).astype(BF16)
            sum_copy(j, n).start()

    def forward_sum(j, n):
        mine = partial(j, n)
        sum_arrival(j + 1, n).wait_recv()
        mine = mine + col_in[j + 1, :, cols(n)].astype(F32)
        col_out[j - 1, :, cols(n)] = mine.astype(BF16)
        sum_copy(j, n).start()

    choose(OWN)
    deal(0, OWN)
    deal(1, OWN)

    halo.wait_recv()
    prod = conv_gate[...].astype(F32) * conv_value[...].astype(F32)
    padded[8:] = prod
    padded[:8] = jnp.where(me == 0, 0.0, halo_dst[...])
    conv = jnp.zeros(prod.shape, F32)
    for tap in range(depth):
        start = 8 - (depth - 1) + tap
        conv = conv + taps[tap : tap + 1] * padded[start : start + toks]
    conv_sum[...] = conv
    mix_src[...] = (gate_in[...].astype(F32) * conv).astype(BF16)

    def mix_copy(j):
        return remote(
            mix_src,
            mix.at[pl.ds(pl.multiple_of(j * toks, toks), toks)],
            m_send.at[0],
            m_recv.at[0],
            (teammate(j), half),
        )

    def mix_all():
        at = mix.at[pl.ds(0, (team - 1) * toks)]
        return remote(at, at, m_send.at[0], m_recv.at[0], (me, other))

    def informed(j):
        table_copy(0, next_layer, j).wait_recv()
        choose(j)

    @pl.when(inner)
    def _():
        relay((0, NEXT, next_to_across), (0, ACROSS, across_to_next))

    @pl.when(outer)
    def _():
        arrived(0, NEXT)

    informed(NEXT)
    deal(0, NEXT)
    for load in loads:
        load.wait()

    @pl.when(inner)
    def _():
        relay((1, NEXT, next_to_across), (0, FAR, far_to_next))
        begin(own_to_across, 1)

    @pl.when(outer)
    def _():
        arrived(1, NEXT)

    deal(1, NEXT)
    ahead(OWN)
    behind(OWN)
    send_back(OWN)

    @pl.when(inner)
    def _():
        relay((1, FAR, far_to_next))

    ahead(NEXT)
    behind(NEXT)
    send_back(NEXT)

    @pl.when(outer)
    def _():
        arrived(0, ACROSS)

    informed(ACROSS)
    deal(0, ACROSS)
    returned(OWN)
    total[...] = dot(pick[OWN], back[group(OWN)], 0, 0)
    returned(NEXT)

    @pl.when(outer)
    def _():
        send_sums(NEXT)
        arrived(0, FAR)

    informed(FAR)
    deal(0, FAR)

    @pl.when(inner)
    def _():
        relay((1, ACROSS, across_to_next))

    ahead(ACROSS)

    @pl.when(outer)
    def _():
        deal_arriving(1, FAR)

    @pl.when(inner)
    def _():
        deal(1, FAR)

    ahead(FAR)

    @pl.when(outer)
    def _():
        deal_arriving(1, ACROSS)

    @pl.when(inner)
    def _():
        deal(1, ACROSS)

    behind(FAR)
    send_back(FAR)
    behind(ACROSS)
    send_back(ACROSS)

    if fused:

        @pl.loop(1, team)
        def _(j):
            mix_copy(j).start()

        mix[pl.ds(0, toks)] = mix_src[...]

    @pl.when(inner)
    def _():
        returned(FAR)

    @pl.when(outer)
    def _():
        send_sums(FAR, True)

    hid_part = hidden.shape[1] // PARTS
    deep_part = width // PARTS

    def weights_part(n):
        to = pl.ds(n * hid_part, hid_part)
        x = hidden[:, to].T
        for h in range(2):
            down_f[to, h * width : (h + 1) * width] = dot(x, cot[h], 1, 0).astype(BF16)

        @pl.loop(0, 2)
        def _(h):
            to = pl.ds(pl.multiple_of(h * width + n * deep_part, deep_part), deep_part)
            x = rows[h, :, n * deep_part : (n + 1) * deep_part].T
            gate_f[to] = dot(x, gg[...], 1, 0).astype(BF16)
            up_f[to] = dot(x, ug[...], 1, 0).astype(BF16)

    for n in range(PARTS):

        @pl.when(inner)
        def _():
            forward_sum(FAR, n)
            if n >= 2:
                forward_sum(NEXT, n - 2)

        weights_part(n)

    stores = [
        pltpu.make_async_copy(gate_f, gate_out.at[0], out_sem.at[0]),
        pltpu.make_async_copy(up_f, up_out.at[0], out_sem.at[1]),
        pltpu.make_async_copy(down_f, down_out.at[0], out_sem.at[2]),
    ]
    for store in stores:
        store.start()

    per = LAYERS // 2
    blk = width // (team * per)

    def band(b):
        return pl.ds(b * blk, blk)

    def spot(h, m, size):
        return pl.ds(pl.multiple_of((h * per + m) * blk, blk), size)

    def stripe(j):
        return pl.ds(pl.multiple_of(j * toks, toks), toks)

    def piece_copy(b, j, m):
        return remote(
            half_out.at[:, band(b)],
            strips.at[stripe(j), spot(half, m, blk)],
            g_send.at[m],
            g_recv.at[m],
            (teammate(j), half),
        )

    def own_piece(b, m):
        return remote(
            half_out.at[:, band(b)],
            strips.at[stripe(0), spot(half, m, blk)],
            own_sem.at[0, m],
            own_sem.at[1, m],
            (me, other),
        )

    def whole_copy(n):
        return remote(
            half_out.at[:, cols(n)], far_half.at[:, cols(n)], b_send.at[0], b_recv.at[0], (me, other)
        )

    def whole_all():
        return remote(half_out, far_half, b_send.at[0], b_recv.at[0], (me, other))

    def handed(j, m):
        at = strips.at[stripe(j), spot(half, m, blk)]
        return remote(at, at, d_send.at[m], d_recv.at[m], (me, other))

    def layer_copy(at):
        return remote(
            share_out.at[at], share_in.at[layer], s_send.at[at], s_recv.at[layer], column(at)
        )

    def layer_arrival(at):
        return remote(
            share_in.at[at], share_in.at[at], s_send.at[at], s_recv.at[at], column(at)
        )

    def hand_over(m):
        pieces_all(m).wait_recv()

        @pl.loop(1, team)
        def _(j):
            handed(j, m).start()

    def pieces_all(m):
        at = strips.at[pl.ds(toks, (team - 1) * toks), band(m)]
        return remote(at, at, g_send.at[m], g_recv.at[m], (me, other))

    def handed_all(m):
        at = strips.at[pl.ds(toks, (team - 1) * toks), band(m)]
        return remote(at, at, d_send.at[m], d_recv.at[m], (me, other))

    def settle(n):
        sum_arrival(0, n).wait_recv()
        now = total[:, cols(n)] + col_in[0, :, cols(n)].astype(F32)
        half_out[:, cols(n)] = (grad_in[:, cols(n)].astype(F32) + now).astype(BF16)
        if fused:
            whole_copy(n).start()
            for b in range(n * share // blk, (n + 1) * share // blk):
                j, m = lax.rem(b % team - place + team, team), b // team

                @pl.when(j > 0)
                def _():
                    piece_copy(b, j, m).start()

                @pl.when(j == 0)
                def _():
                    own_piece(b, m).start()
                    strips[stripe(0), spot(half, m, blk)] = half_out[:, band(b)]

    def settle_inner(n):
        sum_arrival(1, n).wait_recv()
        total[:, cols(n)] += col_in[1, :, cols(n)].astype(F32)
        settle(n)

    @pl.when(outer)
    def _():
        send_sums(ACROSS, True)

    @pl.when(inner)
    def _():
        returned(ACROSS)
        for n in range(PARTS):
            forward_sum(ACROSS, n)
            if n < 2:
                forward_sum(NEXT, PARTS - 2 + n)
            if n >= 2:
                settle_inner(n - 2)
        settle_inner(PARTS - 2)
        if fused:
            hand_over(0)
        settle_inner(PARTS - 1)

    @pl.when(outer)
    def _():
        for n in range(PARTS - 1):
            settle(n)
        if fused:
            hand_over(0)
        settle(PARTS - 1)

    def edge_copy():
        return remote(edge_src, edge_dst, e_sem.at[0], e_sem.at[1], (before, half))

    def mixer_grad():
        mixed = dot(half_out[...], wo[mine_at], 1, 0)
        whole_all().wait_recv()
        mixed = (mixed + dot(far_half[...], wo[other_at], 1, 0)).astype(BF16)
        wide = mixed.astype(F32)
        inner_conv = wide * gate_in[...].astype(F32)
        edge_src[...] = inner_conv[:8]
        edge_copy().start()
        padded[:toks] = inner_conv
        second_out[...] = (wide * conv_sum[...]).astype(BF16)

    def conv_grads():
        edge_copy().wait_recv()
        padded[toks:] = jnp.where(me == count - 1, 0.0, edge_dst[...])
        prod_grad = jnp.zeros((toks, taps.shape[1]), F32)
        for tap in range(depth):
            start = depth - 1 - tap
            prod_grad = prod_grad + taps[tap : tap + 1] * padded[start : start + toks]
        third_out[...] = (prod_grad * conv_value[...].astype(F32)).astype(BF16)
        fourth_out[...] = (prod_grad * conv_gate[...].astype(F32)).astype(BF16)

    def strips_in(m):
        own_piece(0, m).wait_recv()
        handed_all(m).wait_recv()

    def shares_out(m):
        for at in range(m, LAYERS, per):
            now = dot(strips[:, band(at)].T, mix[...], 1, 0)

            @pl.when(layer == at)
            def _():
                first_out[...] = now

            @pl.when(layer != at)
            def _():
                share_out[at] = now.astype(BF16)
                layer_copy(at).start()

    def shares_in():
        for i in (1, 3, 2):
            at = lax.rem(layer + i, LAYERS)
            layer_arrival(at).wait_recv()
            first_out[...] += share_in[at].astype(F32)

    def hopped(which, n):
        at = toks_in.at[which, 0]
        return remote(at, at, z_send.at[which, n], z_recv.at[which, 0, 0], column(next_layer))

    def summed(j):
        at = col_out.at[j - 1]
        return remote(at, at, c_send.at[j - 1], c_recv.at[0, 0], column(next_layer))

    def drain():
        for which in range(2):
            hopped(which, 0).wait_send()
            for j in range(LAYERS):
                passed(which, j).wait_send()
                dealt(which, j).wait_send()

        @pl.when(inner)
        def _():
            for which in range(2):
                for n in range(1, 5):
                    hopped(which, n).wait_send()

        for j in range(LAYERS):
            part_copy(j).wait_send()
            for h in range(2):
                ret_all(j, h).wait_send()

        for j in (NEXT, ACROSS, FAR):
            summed(j).wait_send()
        for copy in tables:
            copy.wait_send()
        halo.wait_send()
        if fused:
            edge_copy().wait_send()
            whole_all().wait_send()
            mix_all().wait_send()
            for m in range(per):
                own_piece(0, m).wait_send()
                handed_all(m).wait_send()
                pieces_all(m).wait_send()

    def keep(n, src, dst):
        stores.append(pltpu.make_async_copy(src, dst, out_sem.at[n]))
        stores[-1].start()

    keep(3, half_out, half_hbm)
    if fused:

        mix_all().wait_recv()
        for m in range(per):
            strips_in(m)
            shares_out(m)
            if m == 0:
                mixer_grad()
            if m + 1 < per:
                hand_over(m + 1)
        conv_grads()
        keep(5, second_out, second_hbm)
        keep(6, third_out, third_hbm)
        keep(7, fourth_out, fourth_hbm)
        drain()
        shares_in()
        keep(4, first_out, first_hbm)
        for i in range(1, LAYERS):
            layer_copy(lax.rem(layer + i, LAYERS)).wait_send()
    else:
        drain()
        keep(4, conv_sum, first_hbm)
        keep(5, mix_src, second_hbm)
        keep(6, halo_src, third_hbm)
        keep(7, halo_dst, fourth_hbm)

    def finish():
        for store in stores:
            store.wait()

    finish()


def expert_pass(
    fused,
    stream,
    out_grad,
    ids,
    weights,
    gate_in,
    conv_gate,
    conv_value,
    taps,
    w_gate,
    w_up,
    w_down,
    w_out,
):
    toks, width = stream.shape
    chans = gate_in.shape[1]
    count = lax.axis_size("sp")
    cap = 4 * toks // count
    team = count // LAYERS
    slots = team * cap
    tall = LAYERS * slots
    deep, hid = w_gate.shape[1:]
    blk = deep // count
    if fused:
        extra = (((blk, chans), F32),) + (((toks, chans), BF16),) * 3
    else:
        extra = (((toks, chans), F32), ((toks, chans), BF16)) + (((8, chans), F32),) * 2
    crew = team if fused else 1
    anywhere = pl.BlockSpec(memory_space=pl.ANY)
    dma = pltpu.SemaphoreType.DMA
    return pl.pallas_call(
        functools.partial(expert_kernel, count, cap, fused),
        out_shape=(
            jax.ShapeDtypeStruct((toks, width), BF16),
            jax.ShapeDtypeStruct((1, deep, hid), BF16),
            jax.ShapeDtypeStruct((1, deep, hid), BF16),
            jax.ShapeDtypeStruct((1, hid, deep), BF16),
        )
        + tuple(jax.ShapeDtypeStruct(*one) for one in extra),
        in_specs=[anywhere] * 12,
        out_specs=(anywhere,) * 8,
        scratch_shapes=[
            pltpu.VMEM((toks, width), BF16),
            pltpu.VMEM((toks, width), BF16),
            pltpu.VMEM(ids.shape, ids.dtype),
            pltpu.VMEM(weights.shape, F32),
            pltpu.VMEM((toks, chans), BF16),
            pltpu.VMEM((toks, chans), BF16),
            pltpu.VMEM((toks, chans), BF16),
            pltpu.VMEM(taps.shape, F32),
            pltpu.VMEM((toks, width), BF16),
            pltpu.VMEM((blk, chans), F32),
            pltpu.VMEM((toks, chans), BF16),
            pltpu.VMEM((toks, chans), BF16),
            pltpu.VMEM((toks, chans), BF16),
            pltpu.VMEM((2, LAYERS - 1, toks, width), BF16),
            pltpu.VMEM((LAYERS, 8, toks), F32),
            pltpu.VMEM((LAYERS, slots, toks), BF16),
            pltpu.VMEM((LAYERS, slots, 1), F32),
            pltpu.VMEM((2, LAYERS, slots, width), BF16),
            pltpu.VMEM((2, tall, width), BF16),
            pltpu.VMEM((2, tall, width), BF16),
            pltpu.VMEM((deep, hid), BF16),
            pltpu.VMEM((deep, hid), BF16),
            pltpu.VMEM((hid, deep), BF16),
            pltpu.VMEM((tall, hid), F32),
            pltpu.VMEM((tall, hid), F32),
            pltpu.VMEM((tall, hid), BF16),
            pltpu.VMEM((tall, hid), BF16),
            pltpu.VMEM((tall, hid), BF16),
            pltpu.VMEM((tall, width), BF16),
            pltpu.VMEM((tall, width), BF16),
            pltpu.VMEM((tall, width), BF16),
            pltpu.VMEM((tall, width), BF16),
            pltpu.VMEM((LAYERS - 1, toks, width), BF16),
            pltpu.VMEM((5, toks, width), BF16),
            pltpu.VMEM((toks, width), F32),
            pltpu.VMEM((deep, hid), BF16),
            pltpu.VMEM((deep, hid), BF16),
            pltpu.VMEM((hid, deep), BF16),
            pltpu.VMEM((crew * toks, chans), BF16),
            pltpu.VMEM((toks, chans), BF16),
            pltpu.VMEM((toks + 8, chans), F32),
            pltpu.VMEM((toks, chans), F32),
            pltpu.VMEM((8, chans), F32),
            pltpu.VMEM((8, chans), F32),
            pltpu.VMEM((deep, chans) if fused else (16, 128), BF16),
            pltpu.VMEM((toks, width) if fused else (16, 128), BF16),
            pltpu.VMEM((team * toks, LAYERS * blk) if fused else (16, 128), BF16),
            pltpu.VMEM((LAYERS, blk, chans), BF16),
            pltpu.VMEM((LAYERS, blk, chans), BF16),
            pltpu.VMEM((8, chans), F32),
            pltpu.VMEM((8, chans), F32),
            dma((8,)),
            dma((4,)),
            dma((8,)),
            dma((2, 5)),
            dma((2, LAYERS - 1, CHUNKS)),
            dma((3,)),
            dma((LAYERS,)),
            dma((2, LAYERS)),
            dma((2, LAYERS, team)),
            dma((2, LAYERS)),
            dma((2, LAYERS)),
            dma((LAYERS,)),
            dma((LAYERS,)),
            dma((LAYERS, 2)),
            dma((LAYERS, 2)),
            dma((LAYERS - 1,)),
            dma((5, PARTS)),
            dma((1,)),
            dma((1,)),
            dma((2,)),
            dma((LAYERS // 2,)),
            dma((LAYERS // 2,)),
            dma((2, LAYERS // 2)),
            dma((LAYERS // 2,)),
            dma((LAYERS // 2,)),
            dma((LAYERS,)),
            dma((LAYERS,)),
            dma((1,)),
            dma((1,)),
            dma((2,)),
        ],
        compiler_params=pltpu.CompilerParams(
            collective_id=0, has_side_effects=True, vmem_limit_bytes=62 * 1024 * 1024
        ),
    )(
        stream,
        out_grad,
        ids,
        weights,
        gate_in,
        conv_gate,
        conv_value,
        taps,
        w_gate,
        w_up,
        w_down,
        w_out,
    )


def publish_kernel(small, large, *refs):
    total = small + large
    ins, outs, refs = refs[:total], refs[total : 2 * total], refs[2 * total :]
    held, wide, (in_sem, out_sem) = refs[:total], refs[total : total + large], refs[total + large :]

    def spots(k):
        if k < small:
            return [(0, slice(None), slice(None))]
        size = held[k].shape[0] // PARTS
        return [(n, (0, pl.ds(n * size, size)), pl.ds(n * size, size)) for n in range(PARTS)]

    def load(k, n, outer_at, at):
        src = ins[k] if k < small else ins[k].at[outer_at]
        dst = held[k] if k < small else held[k].at[at]
        return pltpu.make_async_copy(src, dst, in_sem.at[k, n])

    def store(k, n, outer_at, at):
        src = held[k] if k < small else wide[k - small].at[at]
        dst = outs[k] if k < small else outs[k].at[outer_at]
        return pltpu.make_async_copy(src, dst, out_sem.at[k, n])

    order = list(range(small, total)) + list(range(small))
    steps = [(k, *spot) for k in order for spot in spots(k)]
    for step in steps:
        load(*step).start()
    for step in steps:
        load(*step).wait()
        k, at = step[0], step[3]
        if k >= small:
            wide[k - small][at] = held[k][at].astype(F32)
        store(*step).start()
    for step in steps:
        store(*step).wait()


def publish(smalls, larges):
    anywhere = pl.BlockSpec(memory_space=pl.ANY)
    dma = pltpu.SemaphoreType.DMA
    total = len(smalls) + len(larges)
    outs = [jax.ShapeDtypeStruct(x.shape, x.dtype) for x in smalls]
    outs += [jax.ShapeDtypeStruct(x.shape, F32) for x in larges]
    return pl.pallas_call(
        functools.partial(publish_kernel, len(smalls), len(larges)),
        out_shape=tuple(outs),
        in_specs=[anywhere] * total,
        out_specs=(anywhere,) * total,
        scratch_shapes=[pltpu.VMEM(x.shape, x.dtype) for x in smalls]
        + [pltpu.VMEM(x.shape[1:], BF16) for x in larges]
        + [pltpu.VMEM(x.shape[1:], F32) for x in larges]
        + [dma((total, PARTS)), dma((total, PARTS))],
        compiler_params=pltpu.CompilerParams(vmem_limit_bytes=62 * 1024 * 1024),
    )(*smalls, *larges)


def shards(
    stream,
    out_grad,
    gate_in,
    conv_gate,
    conv_value,
    taps,
    w_out,
    route_ids,
    route_weights,
    w_gate,
    w_up,
    w_down,
):
    tok_rows, channels = conv_gate.shape
    me = lax.axis_index("sp")
    depth = taps.shape[0]
    fused = w_out.shape[0] // lax.axis_size("sp") % 128 == 0
    stream_half, gate_w_grad, up_w_grad, down_w_grad, *extra = expert_pass(
        fused,
        stream,
        out_grad,
        route_ids.T,
        route_weights.T,
        gate_in,
        conv_gate,
        conv_value,
        taps,
        w_gate,
        w_up,
        w_down,
        w_out,
    )
    if fused:
        out_proj_grad, *chan_grads = extra
        smalls = (stream_half, *chan_grads, out_proj_grad)
        return publish(smalls, (gate_w_grad, up_w_grad, down_w_grad))
    conv_sum, mixer_out = extra[:2]
    stream_whole = lax.all_gather(stream_half, "tp", axis=1, tiled=True)
    mixer_grad = dot(stream_whole, w_out, 1, 0).astype(BF16)
    out_proj_grad = lax.psum_scatter(
        dot(stream_whole, mixer_out, 0, 0).astype(BF16), "sp", scatter_dimension=0, tiled=True
    ).astype(F32)
    first = mixer_grad[: depth - 1].astype(F32) * gate_in[: depth - 1].astype(F32)
    halo = passed_along(first, "sp", -1)
    mixer_wide = mixer_grad.astype(jnp.float32)
    gate_in_grad = (mixer_wide * conv_sum).astype(jnp.bfloat16)
    conv_inner = mixer_wide * gate_in.astype(jnp.float32)
    right_rows = jnp.where(me == lax.axis_size("sp") - 1, 0.0, halo[: depth - 1])
    padded_back = jnp.concatenate([conv_inner, right_rows], axis=0)
    prod_grad = jnp.zeros((tok_rows, channels), jnp.float32)
    for tap_index in range(depth):
        offset = depth - 1 - tap_index
        prod_grad = prod_grad + taps[tap_index][None, :] * padded_back[offset : offset + tok_rows]
    conv_gate_grad = (prod_grad * conv_value.astype(jnp.float32)).astype(jnp.bfloat16)
    conv_value_grad = (prod_grad * conv_gate.astype(jnp.float32)).astype(jnp.bfloat16)
    return (
        stream_half,
        gate_in_grad,
        conv_gate_grad,
        conv_value_grad,
        out_proj_grad,
        gate_w_grad.astype(F32),
        up_w_grad.astype(F32),
        down_w_grad.astype(F32),
    )


def solution(mesh):
    placed = (
        P("sp", "tp"),
        P("sp", "tp"),
        P("sp", "tp"),
        P("sp", "tp"),
        P("sp", "tp"),
        P(None, "tp"),
        P(None, "tp"),
        P("sp", None),
        P("sp", None),
        P("sp", None, "tp"),
        P("sp", None, "tp"),
        P("sp", "tp", None),
    )
    return jax.shard_map(
        shards,
        mesh=mesh,
        in_specs=placed,
        out_specs=(
            P("sp", "tp"),
            P("sp", "tp"),
            P("sp", "tp"),
            P("sp", "tp"),
            P("sp", "tp"),
            P("sp", None, "tp"),
            P("sp", None, "tp"),
            P("sp", "tp", None),
        ),
        check_vma=False,
    )
```
